256 devices in a mesh: fs: 32 (over z, x), rep: 4 (over y), tp: 2 (over core).
Axes of the slice: x: 4, y: 4, z: 8, core: 2. Of those that a mesh axis runs over, the one named last changes fastest.
Arguments:
- saved_input: bfloat16 [131072, 2048], P(('fs', 'rep')), may hold values from -500 to 500
- query_cotangent: bfloat16 [131072, 2048], P(('fs', 'rep'), 'tp'), may hold values from -0.0049438477 to 0.0049438477
- key_cotangent: bfloat16 [131072, 512], P(('fs', 'rep'), 'tp'), may hold values from -0.0049438477 to 0.0049438477
- query_weight: float32 [2048, 2048], P('fs', 'tp'), may hold values from -45 to 45
- key_weight: float32 [2048, 512], P('fs', 'tp'), may hold values from -45 to 45
- query_moment: float32 [2048, 2048], P('fs', 'tp'), may hold values from -45 to 45
- key_moment: float32 [2048, 512], P('fs', 'tp'), may hold values from -45 to 45
- query_row_root: bfloat16 [2048, 2048], P('fs'), may hold values from -1 to 3, as said below
- key_row_root: bfloat16 [2048, 2048], P('fs'), may hold values from -1 to 3, as said below
- query_head_root: bfloat16 [32, 64, 64], P('tp'), may hold values from -1 to 3, as said below
- key_head_root: bfloat16 [8, 64, 64], P('tp'), may hold values from -1 to 3, as said below
- query_head_stat: float32 [32, 64, 64], P('tp'), may hold values from -26 to 27, as said below
- key_head_stat: float32 [8, 64, 64], P('tp'), may hold values from -26 to 27, as said below
Outputs:
- query_step: float32 [2048, 2048], P('fs', 'tp')
- key_step: float32 [2048, 512], P('fs', 'tp')
- query_next: float32 [2048, 2048], P('fs', 'tp')
- key_next: float32 [2048, 512], P('fs', 'tp')
- query_copy: bfloat16 [2048, 2048], P(None, 'tp')
- key_copy: bfloat16 [2048, 512], P(None, 'tp')
- query_moment_next: float32 [2048, 2048], P('fs', 'tp')
- key_moment_next: float32 [2048, 512], P('fs', 'tp')
- query_stat_next: float32 [32, 64, 64], P('tp')
- key_stat_next: float32 [8, 64, 64], P('tp')
The draws below stay inside these ranges and needn't reach their ends.
Inputs may be any that keep to these rules, and one draw needn't show every extreme that they name: `query_row_root`: symmetric. `key_row_root`: symmetric. `query_head_root`: each head's matrix is symmetric. `key_head_root`: each head's matrix is symmetric. `query_head_stat`: each head's matrix is symmetric. `key_head_stat`: each head's matrix is symmetric.
All inputs are finite; a program needn't handle non-finite values.
Results may differ from the reference program's by a relative error of at most 0.0018.
The reference program's roundings to bfloat16 on the way count: a program that leaves them out, or rounds other values in their place, can miss the bound.
Values may be sent and summed in bfloat16 or wider, within the bound.
A program may use at most 128 MiB of HBM per device.

```python
import math
import jax
import jax.numpy as jnp
from jax import lax

D = 2048
HEAD_DIM = 64
QHEADS = 32
KVHEADS = 8
TOKENS = 131072
QW = 2048
KW = 512


def rising_scale(length):
    return jnp.exp(jnp.linspace(math.log(0.3), math.log(3.0), length)).astype(jnp.float32)


def column_rise(length):
    return jnp.exp(jnp.linspace(0.0, math.log(10.0), length)).astype(jnp.float32)


def bounded_entries(rng_key, shape):
    return jax.random.truncated_normal(rng_key, -5.0, 5.0, shape, jnp.float32)


def matrix_draw(key, marker, row_total, col_total):
    first_key, second_key = jax.random.split(jax.random.fold_in(key, marker))
    entries = bounded_entries(first_key, (row_total, col_total))
    col_scale = jnp.exp(jax.random.uniform(second_key, (1, col_total), jnp.float32, math.log(0.3), math.log(3.0)))
    return entries * rising_scale(row_total)[:, None] * col_scale


def root_draw(key, marker, count_mats, order):
    first_key, second_key = jax.random.split(jax.random.fold_in(key, marker))
    diagonal = jnp.exp(jax.random.uniform(first_key, (count_mats, order), jnp.float32, math.log(0.5), math.log(2.0)))
    off_diagonal = bounded_entries(second_key, (count_mats, order, order)) * (0.7 / math.sqrt(order))
    symmetric = 0.5 * (off_diagonal + jnp.swapaxes(off_diagonal, 1, 2))
    identity = jnp.eye(order, dtype=jnp.float32)[None]
    return symmetric * (1.0 - identity) + diagonal[:, :, None] * identity


def stat_draw(key, marker, count_mats):
    factor = bounded_entries(jax.random.fold_in(key, marker), (count_mats, HEAD_DIM, HEAD_DIM))
    gram = jnp.einsum('hde,hfe->hdf', factor, factor, precision=jax.lax.Precision.HIGHEST) / HEAD_DIM
    return gram + 0.6 * jnp.eye(HEAD_DIM, dtype=jnp.float32)[None]


def draw_saved_input(key, part):
    first_key, second_key = jax.random.split(jax.random.fold_in(key, 101))
    entries = bounded_entries(first_key, (TOKENS, D))
    token_scale = jnp.exp(jax.random.uniform(second_key, (TOKENS, 1), jnp.float32, 0.0, math.log(10.0)))
    return (entries * token_scale * column_rise(D)[None, :]).astype(jnp.bfloat16)


def draw_query_weight(key, part):
    return matrix_draw(key, 201, D, QHEADS * HEAD_DIM)


def draw_key_weight(key, part):
    return matrix_draw(key, 202, D, KVHEADS * HEAD_DIM)


def draw_query_moment(key, part):
    return matrix_draw(key, 203, D, QHEADS * HEAD_DIM)


def draw_key_moment(key, part):
    return matrix_draw(key, 204, D, KVHEADS * HEAD_DIM)


def draw_query_row_root(key, part):
    return root_draw(key, 301, 1, D)[0].astype(jnp.bfloat16)


def draw_key_row_root(key, part):
    return root_draw(key, 302, 1, D)[0].astype(jnp.bfloat16)


def draw_query_head_root(key, part):
    return root_draw(key, 303, QHEADS, HEAD_DIM).astype(jnp.bfloat16)


def draw_key_head_root(key, part):
    return root_draw(key, 304, KVHEADS, HEAD_DIM).astype(jnp.bfloat16)


def draw_query_head_stat(key, part):
    return stat_draw(key, 401, QHEADS)


def draw_key_head_stat(key, part):
    return stat_draw(key, 402, KVHEADS)


def block_levels(rng, extent, cuts, smallest, largest):
    loudness = 1.0
    for axis_at, parts in cuts:
        heights = jax.random.uniform(jax.random.fold_in(jax.random.fold_in(rng, 6), axis_at), (parts,), jnp.float32, smallest / len(cuts), largest / len(cuts))
        loudness = loudness * jnp.repeat(jnp.exp(heights), extent[axis_at] // parts).reshape((-1,) + (1,) * (len(extent) - 1 - axis_at))
    return loudness


def normal_values(key, extent, spread, most, cuts=(), kind=jnp.bfloat16):
    factor_of = block_levels(key, extent, cuts, -0.22, 0.18) if cuts else 1.0
    array = jax.random.normal(key, extent, jnp.float32) * spread * factor_of
    return jnp.minimum(jnp.maximum(array, -most), most).astype(kind)


def setup_inputs(seed: int = 0) -> dict:
    seeds = jax.random.split(jax.random.key(seed), 14)
    saved_input = draw_saved_input(jax.random.fold_in(seeds[13], 71), 0)
    query_cotangent = normal_values(seeds[1], (TOKENS, QW), (0.3 / TOKENS ** 0.5), 0.0049438477, ((0, 128), (1, 2)))
    key_cotangent = normal_values(seeds[2], (TOKENS, KW), (0.3 / TOKENS ** 0.5), 0.0049438477, ((0, 128), (1, 2)))
    query_weight = draw_query_weight(jax.random.fold_in(seeds[13], 71), 0)
    key_weight = draw_key_weight(jax.random.fold_in(seeds[13], 71), 0)
    query_moment = draw_query_moment(jax.random.fold_in(seeds[13], 71), 0)
    key_moment = draw_key_moment(jax.random.fold_in(seeds[13], 71), 0)
    query_row_root = draw_query_row_root(jax.random.fold_in(seeds[13], 71), 0)
    key_row_root = draw_key_row_root(jax.random.fold_in(seeds[13], 71), 0)
    query_head_root = draw_query_head_root(jax.random.fold_in(seeds[13], 71), 0)
    key_head_root = draw_key_head_root(jax.random.fold_in(seeds[13], 71), 0)
    query_head_stat = draw_query_head_stat(jax.random.fold_in(seeds[13], 71), 0)
    key_head_stat = draw_key_head_stat(jax.random.fold_in(seeds[13], 71), 0)
    return dict(saved_input=saved_input, query_cotangent=query_cotangent, key_cotangent=key_cotangent, query_weight=query_weight, key_weight=key_weight, query_moment=query_moment, key_moment=key_moment, query_row_root=query_row_root, key_row_root=key_row_root, query_head_root=query_head_root, key_head_root=key_head_root, query_head_stat=query_head_stat, key_head_stat=key_head_stat)


MOMENT_DECAY = 0.8
STAT_DECAY = 0.5
LEARN_RATE = 0.1
EPSILON = 1e-06

def update(gradient, weight, moment, stat, row_root, head_root):
    row_total = gradient.shape[0]
    head_count = head_root.shape[0]
    rounded = lax.optimization_barrier(gradient.astype(jnp.bfloat16)).astype(jnp.float32)
    shaped = rounded.reshape(row_total, head_count, HEAD_DIM)
    gram = jnp.einsum('rhd,rhe->hde', shaped, shaped)
    stat_next = STAT_DECAY * stat + (1.0 - STAT_DECAY) * gram / D
    rightward = jnp.einsum('rhd,hde->rhe', shaped, head_root.astype(jnp.float32))
    rightward = rightward.reshape(row_total, head_count * HEAD_DIM).astype(jnp.bfloat16)
    preconditioned = jnp.dot(row_root, rightward, preferred_element_type=jnp.float32)
    moment_next = MOMENT_DECAY * moment + (1.0 - MOMENT_DECAY) * preconditioned
    trust_ratio = jnp.sqrt(jnp.sum(weight * weight)) / jnp.sqrt(jnp.sum(moment_next * moment_next) + EPSILON)
    update_step = LEARN_RATE * trust_ratio * moment_next
    weight_next = weight - update_step
    return (update_step, weight_next, weight_next.astype(jnp.bfloat16), moment_next, stat_next)

def token_sum(saved_input, cotangent):
    return lax.dot_general(saved_input, cotangent, (((0,), (0,)), ((), ())), preferred_element_type=jnp.float32)

def reference(saved_input, query_cotangent, key_cotangent, query_weight, key_weight, query_moment, key_moment, query_row_root, key_row_root, query_head_root, key_head_root, query_head_stat, key_head_stat):
    query_out = update(token_sum(saved_input, query_cotangent), query_weight, query_moment, query_head_stat, query_row_root, query_head_root)
    key_out = update(token_sum(saved_input, key_cotangent), key_weight, key_moment, key_head_stat, key_row_root, key_head_root)
    return (query_out[0], key_out[0], query_out[1], key_out[1], query_out[2], key_out[2], query_out[3], key_out[3], query_out[4], key_out[4])
```

```python
import functools

import jax
import jax.numpy as jnp
from jax import lax
from jax.experimental import pallas as pl
from jax.experimental.pallas import tpu as pltpu
from jax.sharding import Mesh
from jax.sharding import PartitionSpec as P

D = 2048
HEAD_DIM = 64
NZ, NX, NY = 8, 4, 4
Z, X, Y = "fs_0", "fs_1", "rep"
FS = (Z, X)
FS_TP = (Z, X, "tp")
FS_REP = (Z, X, Y)
ROWS = (Y, X, Z)
MOMENT_DECAY = 0.8
STAT_DECAY = 0.5
LEARN_RATE = 0.1
EPSILON = 1e-06
MESH = pl.DeviceIdType.MESH
WA, WB, WC = 512, 384, 384
BLK = 16


def plane_pairs():
    return [(dy, dx) for dy in range(NY) for dx in range(NX) if dy or dx]


def greet(peers):
    barrier = pltpu.get_barrier_semaphore()
    for dev in peers:
        pl.semaphore_signal(barrier, inc=1, device_id=dev, device_id_type=MESH)
    pl.semaphore_wait(barrier, len(peers))


def ring_slots(n):
    slots = [(n // 2, 0, None)]
    for k in range(1, n // 2):
        slots.append((n // 2 - k, 1, 2 * k - 3 if k >= 2 else None))
        slots.append((n // 2 - k, 0, 2 * k - 2))
    return slots


class Ring:
    def __init__(self, axis, n, region, recv, send_sem, recv_sem, add):
        self.n, self.me = n, lax.axis_index(axis)
        self.region, self.recv, self.add = region, recv, add
        self.slots = ring_slots(n)
        self.copies = {}
        for way in range(2):
            to = lax.rem(self.me + (1 if way == 0 else n - 1), n)
            for j, (dist, half, _) in enumerate(self.slots):
                self.copies[way, j] = pltpu.make_async_remote_copy(
                    src_ref=region(self.chunk(way, dist), half ^ way),
                    dst_ref=recv.at[way, j],
                    send_sem=send_sem.at[way, j],
                    recv_sem=recv_sem.at[way, j],
                    device_id={axis: to},
                    device_id_type=MESH,
                )

    def chunk(self, way, dist):
        return lax.rem(self.me + (dist if way == 0 else self.n - dist), self.n)

    def send(self, j):
        for way in range(2):
            dist, half, source = self.slots[j]
            if source is not None:
                self.copies[way, source].wait_recv()
                self.add(self.chunk(way, dist), half ^ way, self.recv.at[way, source])
            self.copies[way, j].start()

    def finish(self):
        for j in (self.n - 3, self.n - 2):
            for way in range(2):
                self.copies[way, j].wait_recv()
                self.add(self.me, self.slots[j][1] ^ way, self.recv.at[way, j])

    def drain(self):
        for copy in self.copies.values():
            copy.wait_send()


def gradient_kernel(
    x_ref, qc_ref, kc_ref, out_ref,
    ga, gb, gc, ra, rb, rc, pa, b1, c1, b2, c2,
    a_ss, a_rs, b_ss, b_rs, c_ss, c_rs, pa_ss, pa_rs, b1_ss, b1_rs, c1_ss, c1_rs, b2_ss, b2_rs, c2_ss, c2_rs,
):
    z, x, y = lax.axis_index(Z), lax.axis_index(X), lax.axis_index(Y)
    z_of = [lax.rem(z + d, NZ) for d in range(NZ)]
    x_of = [lax.rem(x + d, NX) for d in range(NX)]
    y_of = [lax.rem(y + d, NY) for d in range(NY)]
    greet(
        [{Z: z_of[d]} for d in range(1, NZ)]
        + [{Y: y_of[dy], X: x_of[dx]} for dy, dx in plane_pairs()]
    )

    def product(start, count, cot, low, width):
        return lax.dot_general(
            x_ref[:, pl.ds(pl.multiple_of(start, 128), count)],
            cot[:, low : low + width],
            (((0,), (0,)), ((), ())),
            preferred_element_type=jnp.float32,
        )

    def add_a(chunk, half, recv):
        for y2 in range(2):
            def body(x2, _):
                at = (2 * half + y2, x2, chunk)
                ga[at] = ga[at] + recv[y2, x2]
                return 0
            lax.fori_loop(0, NX, body, 0)

    def add_b(chunk, half, recv):
        for y2 in range(2):
            def body(z2, _):
                at = (2 * half + y2, chunk, z2)
                gb[at] = gb[at] + recv[y2, z2]
                return 0
            lax.fori_loop(0, NZ, body, 0)

    def add_c(chunk, half, recv):
        for x2 in range(2):
            def body(z2, _):
                at = (chunk, 2 * half + x2, z2)
                gc[at] = gc[at] + recv[x2, z2]
                return 0
            lax.fori_loop(0, NZ, body, 0)

    ring_a = Ring(Z, NZ, lambda c, h: ga.at[pl.ds(2 * h, 2), :, c], ra, a_ss, a_rs, add_a)
    ring_b = Ring(X, NX, lambda c, h: gb.at[pl.ds(2 * h, 2), c], rb, b_ss, b_rs, add_b)
    ring_c = Ring(Y, NY, lambda c, h: gc.at[c, pl.ds(2 * h, 2)], rc, c_ss, c_rs, add_c)

    def make_a(yy, _):
        ga[yy] = product(yy * 512, 512, qc_ref, 0, WA).reshape(NX, NZ, BLK, WA)
        return 0

    def make_b(chunk):
        def body(yy, _):
            gb[yy, chunk] = product(yy * 512 + chunk * 128, 128, qc_ref, WA, WB).reshape(NZ, BLK, WB)
            return 0
        lax.fori_loop(0, NY, body, 0)

    def make_c(chunk):
        gc[chunk, :, :, :, 0:128] = product(chunk * 512, 512, qc_ref, WA + WB, 128).reshape(NX, NZ, BLK, 128)
        gc[chunk, :, :, :, 128:WC] = product(chunk * 512, 512, kc_ref, 0, 256).reshape(NX, NZ, BLK, 256)

    lax.fori_loop(0, NY, make_a, 0)
    ring_a.send(0)
    ring_a.send(1)
    make_b(x_of[2])
    ring_b.send(0)
    make_c(y_of[2])
    ring_c.send(0)
    make_b(x_of[1])
    make_b(x_of[3])
    ring_b.send(1)
    make_c(y_of[1])
    make_c(y_of[3])
    ring_c.send(1)
    ring_a.send(2)
    make_b(x_of[0])
    make_c(y_of[0])
    ring_a.send(3)
    ring_b.send(2)
    ring_c.send(2)
    ring_a.send(4)
    ring_a.send(5)
    ring_a.send(6)

    def direct(src, dst, ss, rs, d, dev):
        return pltpu.make_async_remote_copy(
            src_ref=src, dst_ref=dst.at[d], send_sem=ss.at[d], recv_sem=rs.at[d],
            device_id=dev, device_id_type=MESH,
        )

    ring_c.finish()
    to_c1 = [direct(gc.at[y, x_of[d]], c1, c1_ss, c1_rs, d - 1, {X: x_of[d]}) for d in (1, 3, 2)]
    for copy in to_c1:
        copy.start()
    ring_b.finish()
    to_b1 = [direct(gb.at[y_of[d], x], b1, b1_ss, b1_rs, d - 1, {Y: y_of[d]}) for d in (1, 3, 2)]
    for copy in to_b1:
        copy.start()

    for copy in to_c1:
        copy.wait_recv()
    def sum_c(zz, _):
        gc[y, x, zz] = (gc[y, x, zz] + c1[0, zz]) + (c1[1, zz] + c1[2, zz])
        return 0
    lax.fori_loop(0, NZ, sum_c, 0)
    to_c2 = [direct(gc.at[y, x, z_of[d]], c2, c2_ss, c2_rs, d - 1, {Z: z_of[d]}) for d in range(1, NZ)]
    for copy in to_c2:
        copy.start()

    ring_a.finish()
    to_pa = [
        direct(ga.at[y_of[dy], x_of[dx], z], pa, pa_ss, pa_rs, i, {Y: y_of[dy], X: x_of[dx]})
        for i, (dy, dx) in enumerate(plane_pairs())
    ]
    for copy in to_pa:
        copy.start()

    for copy in to_b1:
        copy.wait_recv()
    def sum_b(zz, _):
        gb[y, x, zz] = (gb[y, x, zz] + b1[0, zz]) + (b1[1, zz] + b1[2, zz])
        return 0
    lax.fori_loop(0, NZ, sum_b, 0)
    to_b2 = [direct(gb.at[y, x, z_of[d]], b2, b2_ss, b2_rs, d - 1, {Z: z_of[d]}) for d in range(1, NZ)]
    for copy in to_b2:
        copy.start()

    for copy in to_c2:
        copy.wait_recv()
    total = gc[y, x, z]
    for d in range(NZ - 1):
        total = total + c2[d]
    out_ref[:, WA + WB :] = total
    for copy in to_pa:
        copy.wait_recv()
    total = ga[y, x, z]
    for d in range(NX * NY - 1):
        total = total + pa[d]
    out_ref[:, :WA] = total
    for copy in to_b2:
        copy.wait_recv()
    total = gb[y, x, z]
    for d in range(NZ - 1):
        total = total + b2[d]
    out_ref[:, WA : WA + WB] = total

    for ring in (ring_a, ring_b, ring_c):
        ring.drain()
    for copy in to_c1 + to_b1 + to_c2 + to_pa + to_b2:
        copy.wait_send()


def gradient_block(x, qc, kc):
    f32, dma = jnp.float32, pltpu.SemaphoreType.DMA
    vm = pltpu.VMEM
    space = pl.BlockSpec(memory_space=pltpu.VMEM)
    sems = []
    for shape in ((2, 7), (2, 3), (2, 3), (15,), (3,), (3,), (7,), (7,)):
        sems += [dma(shape), dma(shape)]
    return pl.pallas_call(
        gradient_kernel,
        out_shape=jax.ShapeDtypeStruct((BLK, WA + WB + WC), f32),
        in_specs=[space] * 3,
        out_specs=space,
        scratch_shapes=[
            vm((NY, NX, NZ, BLK, WA), f32),
            vm((NY, NX, NZ, BLK, WB), f32),
            vm((NY, NX, NZ, BLK, WC), f32),
            vm((2, 7, 2, NX, BLK, WA), f32),
            vm((2, 3, 2, NZ, BLK, WB), f32),
            vm((2, 3, 2, NZ, BLK, WC), f32),
            vm((15, BLK, WA), f32),
            vm((3, NZ, BLK, WB), f32),
            vm((3, NZ, BLK, WC), f32),
            vm((7, BLK, WB), f32),
            vm((7, BLK, WC), f32),
        ] + sems,
        compiler_params=pltpu.CompilerParams(
            collective_id=0, has_side_effects=True, vmem_limit_bytes=60 * 2**20
        ),
        name="gradient_sum",
    )(x, qc, kc)


def head_gram(rounded, head_count):
    shaped = rounded.reshape(rounded.shape[0], head_count, HEAD_DIM)
    return jnp.einsum("rhd,rhe->hde", shaped, shaped, preferred_element_type=jnp.float32)


def column_factor(rounded, head_root):
    head_count = head_root.shape[0]
    shaped = rounded.reshape(rounded.shape[0], head_count, HEAD_DIM)
    rightward = jnp.einsum("rhd,hde->rhe", shaped, head_root, preferred_element_type=jnp.float32)
    return rightward.reshape(rounded.shape[0], head_count * HEAD_DIM).astype(jnp.bfloat16)


def shards(x, qc, kc, qw, kw, qm, km, ql, kl, qr, kr, qs, ks):
    qn = qc.shape[1]
    grad = gradient_block(x, qc, kc)
    rounded = grad.astype(jnp.bfloat16)
    root = jnp.concatenate([qr, kr], axis=0)
    right = column_factor(rounded, root)
    piece = lax.all_gather(right, ROWS, axis=0, tiled=True)
    gram = lax.psum(head_gram(rounded, root.shape[0]), ROWS)
    hq = qr.shape[0]
    qs2 = STAT_DECAY * qs + (1.0 - STAT_DECAY) * gram[:hq] / D
    ks2 = STAT_DECAY * ks + (1.0 - STAT_DECAY) * gram[hq:] / D
    qp = jnp.dot(ql, piece[:, :qn], preferred_element_type=jnp.float32)
    kp = jnp.dot(kl, piece[:, qn:], preferred_element_type=jnp.float32)
    qm2 = MOMENT_DECAY * qm + (1.0 - MOMENT_DECAY) * qp
    km2 = MOMENT_DECAY * km + (1.0 - MOMENT_DECAY) * kp
    sums = jnp.stack([jnp.sum(qw * qw), jnp.sum(qm2 * qm2), jnp.sum(kw * kw), jnp.sum(km2 * km2)])
    n = lax.axis_size(FS_TP)
    every = lax.all_to_all(jnp.broadcast_to(sums[None], (n, 4)), FS_TP, 0, 0, tiled=True).sum(axis=0)
    qstep = LEARN_RATE * (jnp.sqrt(every[0]) / jnp.sqrt(every[1] + EPSILON)) * qm2
    kstep = LEARN_RATE * (jnp.sqrt(every[2]) / jnp.sqrt(every[3] + EPSILON)) * km2
    qn2 = qw - qstep
    kn2 = kw - kstep
    both = jnp.concatenate([qn2, kn2], axis=1).astype(jnp.bfloat16)
    mine = lax.dynamic_slice_in_dim(both, lax.axis_index(Y) * BLK, BLK, 0)
    copy = lax.all_gather(mine, FS_REP, axis=0, tiled=True)
    return qstep, kstep, qn2, kn2, copy[:, :qn], copy[:, qn:], qm2, km2, qs2, ks2


def solution(mesh):
    split = Mesh(
        mesh.devices.reshape(NZ, NX, NY, mesh.shape["tp"]), (Z, X, Y, "tp")
    )
    row = P(FS, "tp")
    head = P("tp", None, None)
    whole = P(None, "tp")
    tok = P(FS_REP, "tp")
    return jax.shard_map(
        shards, mesh=split,
        in_specs=(P(FS_REP, None), tok, tok, row, row, row, row, P(FS, None), P(FS, None), head, head, head, head),
        out_specs=(row, row, row, row, whole, whole, row, row, head, head),
        check_vma=False,
    )
```

```python
import jax
import jax.numpy as jnp
from jax import lax
from jax.experimental import pallas as pl
from jax.experimental.pallas import tpu as pltpu
from jax.sharding import Mesh
from jax.sharding import PartitionSpec as P

D = 2048
HEAD_DIM = 64
NZ, NX, NY, NT = 8, 4, 4, 2
Z, X, Y, T = "fs_0", "fs_1", "rep", "tp"
FS = (Z, X)
FS_REP = (Z, X, Y)
MOMENT_DECAY = 0.8
STAT_DECAY = 0.5
LEARN_RATE = 0.1
EPSILON = 1e-06
MESH = pl.DeviceIdType.MESH
QN, KN = 1024, 256
WA, WB, WC = 512, 384, 384
WP = 640
BLK = 16
PAIRS = 10
QPAIRS = 8
COPIES = 256
F32, BF16 = jnp.float32, jnp.bfloat16


class Net:
    def __init__(self, send_sem, recv_sem):
        self.send_sem, self.recv_sem, self.used, self.sent = send_sem, recv_sem, 0, []

    def copy(self, src, dst, dev, landing=None):
        k = self.used
        self.used += 1
        copies = [
            pltpu.make_async_remote_copy(
                src_ref=a, dst_ref=b, send_sem=self.send_sem.at[k], recv_sem=self.recv_sem.at[k],
                device_id=dev, device_id_type=MESH,
            )
            for a, b in ((src, dst), (dst, dst) if landing is None else (landing, landing))
        ]
        return Copy(self, *copies)

    def drain(self):
        for copy in self.sent:
            copy.wait_send()


class Copy:
    def __init__(self, net, out, into):
        self.net, self.out, self.into = net, out, into

    def start(self):
        self.out.start()
        self.net.sent.append(self.out)

    def wait(self):
        self.into.wait_recv()


def start_all(copies):
    for copy in copies:
        copy.start()


def wait_all(copies):
    for copy in copies:
        copy.wait()


class Ring:
    def __init__(self, axis, n):
        self.n, self.me = n, lax.axis_index(axis)
        self.copies = {}
        self.device = [{axis: self.place(way, 1)} for way in range(2)]

    def place(self, way, dist):
        return lax.rem(self.me + (dist if way == 0 else self.n - dist), self.n)


class RingSum(Ring):
    def __init__(self, net, axis, n, region, recv, add):
        super().__init__(axis, n)
        self.recv, self.add = recv, add
        self.slots = [(n // 2, 0, None)]
        for k in range(1, n // 2):
            self.slots.append((n // 2 - k, 1, 2 * k - 3 if k >= 2 else None))
            self.slots.append((n // 2 - k, 0, 2 * k - 2))
        for way in range(2):
            for j, (dist, half, _) in enumerate(self.slots):
                self.copies[way, j] = net.copy(
                    region(self.place(way, dist), half ^ way), recv.at[way, j], self.device[way]
                )

    def send(self, j):
        for way in range(2):
            dist, half, source = self.slots[j]
            if source is not None:
                self.copies[way, source].wait()
                self.add(self.place(way, dist), half ^ way, self.recv.at[way, source])
            self.copies[way, j].start()

    def finish(self):
        for j in (self.n - 3, self.n - 2):
            for way in range(2):
                self.copies[way, j].wait()
                self.add(self.me, self.slots[j][1] ^ way, self.recv.at[way, j])


class RingGather(Ring):
    def __init__(self, net, axis, n, regions):
        super().__init__(axis, n)
        slots = [(j // 2, j % 2) for j in range(n - 1)]
        for way in range(2):
            for j, (k, half) in enumerate(slots):
                held = regions(self.place(1 - way, k), half ^ way)
                coming = regions(self.place(1 - way, k + 1), half ^ way)
                self.copies[way, j] = [
                    net.copy(a, a, self.device[way], b) for a, b in zip(held, coming)
                ]

    def send(self, j):
        for way in range(2):
            if j >= 2:
                wait_all(self.copies[way, j - 2])
            start_all(self.copies[way, j])

    def finish(self):
        for j in (self.n - 3, self.n - 2):
            for way in range(2):
                wait_all(self.copies[way, j])


def lane_sums(value):
    total = value[:, 0:128]
    for i in range(1, value.shape[1] // 128):
        total = total + value[:, 128 * i : 128 * (i + 1)]
    return jnp.sum(total, axis=0, keepdims=True)


def step_kernel(
    x_ref, qc_ref, kc_ref, qw_ref, kw_ref, qm_ref, km_ref, ql_ref, kl_ref, qr_ref, kr_ref, qs_ref, ks_ref,
    qstep_ref, kstep_ref, qnext_ref, knext_ref, qcopy_ref, kcopy_ref, qm2_ref, km2_ref, qs2_ref, ks2_ref,
    ga, gb, gc, ra, rb, rc, pa, b1, c1, b2, c2,
    gath, roots, pp, pr, mbuf, gp, gr, gfin, plane, zed, send_sem, recv_sem,
):
    z, x, y, t = (lax.axis_index(a) for a in (Z, X, Y, T))
    z_of = [lax.rem(z + d, NZ) for d in range(NZ)]
    x_of = [lax.rem(x + d, NX) for d in range(NX)]
    y_of = [lax.rem(y + d, NY) for d in range(NY)]
    spots = [(dy, dx) for dy in range(NY) for dx in range(NX)]
    others = [(dy, dx, dt) for dy, dx in spots for dt in range(NT) if dy or dx or dt]
    net = Net(send_sem, recv_sem)

    peers = [{Z: z_of[d]} for d in range(1, NZ)] + [
        {Y: y_of[dy], X: x_of[dx], T: lax.rem(t + dt, NT)} for dy, dx, dt in others
    ]
    barrier = pltpu.get_barrier_semaphore()
    for dev in peers:
        pl.semaphore_signal(barrier, inc=1, device_id=dev, device_id_type=MESH)
    pl.semaphore_wait(barrier, len(peers))

    def product(start, count, cot, low, width):
        return lax.dot_general(
            x_ref[:, pl.ds(pl.multiple_of(start, 128), count)],
            cot[:, low : low + width],
            (((0,), (0,)), ((), ())),
            preferred_element_type=F32,
        )

    def add_a(chunk, half, recv):
        for y2 in range(2):
            def body(x2, _):
                at = (2 * half + y2, x2, chunk)
                ga[at] = ga[at] + recv[y2, x2]
                return 0
            lax.fori_loop(0, NX, body, 0)

    def add_b(chunk, half, recv):
        for y2 in range(2):
            def body(z2, _):
                at = (2 * half + y2, chunk, z2)
                gb[at] = gb[at] + recv[y2, z2]
                return 0
            lax.fori_loop(0, NZ, body, 0)

    def add_c(chunk, half, recv):
        for x2 in range(2):
            def body(z2, _):
                at = (chunk, 2 * half + x2, z2)
                gc[at] = gc[at] + recv[x2, z2]
                return 0
            lax.fori_loop(0, NZ, body, 0)

    ring_a = RingSum(net, Z, NZ, lambda c, h: ga.at[pl.ds(2 * h, 2), :, c], ra, add_a)
    ring_b = RingSum(net, X, NX, lambda c, h: gb.at[pl.ds(2 * h, 2), c], rb, add_b)
    ring_c = RingSum(net, Y, NY, lambda c, h: gc.at[c, pl.ds(2 * h, 2)], rc, add_c)

    def make_a(yy, _):
        ga[yy] = product(yy * 512, 512, qc_ref, 0, WA).reshape(NX, NZ, BLK, WA)
        return 0

    def make_b(chunk):
        def body(yy, _):
            gb[yy, chunk] = product(yy * 512 + chunk * 128, 128, qc_ref, WA, WB).reshape(NZ, BLK, WB)
            return 0
        lax.fori_loop(0, NY, body, 0)

    def make_c(chunk):
        gc[chunk, :, :, :, 0:128] = product(chunk * 512, 512, qc_ref, WA + WB, 128).reshape(NX, NZ, BLK, 128)
        gc[chunk, :, :, :, 128:WC] = product(chunk * 512, 512, kc_ref, 0, KN).reshape(NX, NZ, BLK, KN)

    lax.fori_loop(0, NY, make_a, 0)
    ring_a.send(0)
    ring_a.send(1)
    make_b(x_of[2])
    ring_b.send(0)
    make_c(y_of[2])
    ring_c.send(0)
    make_b(x_of[1])
    make_b(x_of[3])
    ring_b.send(1)
    make_c(y_of[1])
    make_c(y_of[3])
    ring_c.send(1)
    ring_a.send(2)
    make_b(x_of[0])
    make_c(y_of[0])

    roots[...] = jnp.zeros_like(roots)
    for p in range(PAIRS):
        ref, h = (qr_ref, 2 * p) if p < QPAIRS else (kr_ref, 2 * (p - QPAIRS))
        roots[p, 0:HEAD_DIM, 0:HEAD_DIM] = ref[h]
        roots[p, HEAD_DIM : 2 * HEAD_DIM, HEAD_DIM : 2 * HEAD_DIM] = ref[h + 1]

    ring_a.send(3)
    ring_b.send(2)
    ring_c.send(2)
    ring_a.send(4)
    ring_a.send(5)
    ring_a.send(6)

    ring_c.finish()
    to_c1 = [net.copy(gc.at[y, x_of[d]], c1.at[d - 1], {X: x_of[d]}) for d in (1, 3, 2)]
    start_all(to_c1)
    ring_b.finish()
    to_b1 = [net.copy(gb.at[y_of[d], x], b1.at[d - 1], {Y: y_of[d]}) for d in (1, 3, 2)]
    start_all(to_b1)

    wait_all(to_c1)
    def sum_c(zz, _):
        gc[y, x, zz] = (gc[y, x, zz] + c1[0, zz]) + (c1[1, zz] + c1[2, zz])
        return 0
    lax.fori_loop(0, NZ, sum_c, 0)
    to_c2 = [net.copy(gc.at[y, x, z_of[d]], c2.at[d - 1], {Z: z_of[d]}) for d in range(1, NZ)]
    start_all(to_c2)

    ring_a.finish()
    to_pa = [
        net.copy(ga.at[y_of[dy], x_of[dx], z], pa.at[i], {Y: y_of[dy], X: x_of[dx]})
        for i, (dy, dx) in enumerate(spots[1:])
    ]
    start_all(to_pa)

    wait_all(to_b1)
    def sum_b(zz, _):
        gb[y, x, zz] = (gb[y, x, zz] + b1[0, zz]) + (b1[1, zz] + b1[2, zz])
        return 0
    lax.fori_loop(0, NZ, sum_b, 0)
    to_b2 = [net.copy(gb.at[y, x, z_of[d]], b2.at[d - 1], {Z: z_of[d]}) for d in range(1, NZ)]
    start_all(to_b2)

    mine = gath.at[x, z]

    def settle(own, arrived, low, width):
        total = own
        for d in range(arrived.shape[0]):
            total = total + arrived[d]
        mine[:, low : low + width] = total.astype(BF16)

    wait_all(to_c2)
    settle(gc[y, x, z], c2, WA + WB, WC)
    wait_all(to_pa)
    settle(ga[y, x, z], pa, 0, WA)
    wait_all(to_b2)
    settle(gb[y, x, z], b2, WA, WB)

    p_x = [net.copy(gath.at[x, z, :, 0:WP], gath.at[x, z, :, 0:WP], {X: x_of[d]}, gath.at[x_of[NX - d], z, :, 0:WP]) for d in (1, 3, 2)]
    start_all(p_x)
    q_z = [net.copy(gath.at[x, z, :, WP:], gath.at[x, z, :, WP:], {Z: z_of[d]}, gath.at[x, z_of[NZ - d], :, WP:]) for d in (4, 3, 5, 2, 6, 1, 7)]
    start_all(q_z)
    ring_p = RingGather(net, Z, NZ, lambda c, h: [gath.at[pl.ds(2 * h, 2), c, :, 0:WP]])
    wait_all(p_x)
    ring_p.send(0)
    ring_p.send(1)
    wait_all(q_z)
    q_x = [net.copy(gath.at[x, :, :, WP:], gath.at[x, :, :, WP:], {X: x_of[d]}, gath.at[x_of[NX - d], :, :, WP:]) for d in (1, 3, 2)]
    start_all(q_x)
    for j in range(2, NZ - 1):
        ring_p.send(j)

    l_at = pl.ds(pl.multiple_of(y * 512, 512), 512)

    def tile(p):
        return gath[:, :, :, 128 * p : 128 * (p + 1)].reshape(NX * NZ * BLK, 128)

    def precondition(p):
        right = jnp.dot(tile(p), roots[p], preferred_element_type=F32).astype(BF16)
        left = ql_ref if p < QPAIRS else kl_ref
        part = jnp.dot(left[:, l_at], right, preferred_element_type=F32)
        pp[:, :, 128 * p : 128 * (p + 1)] = part.reshape(NY, BLK, 128)

    wait_all(q_x)
    for p in range(WP // 128, PAIRS):
        precondition(p)
    ring_p.finish()
    for p in range(WP // 128):
        precondition(p)

    to_pr = [net.copy(pp.at[y_of[d]], pr.at[d - 1], {Y: y_of[d]}) for d in (1, 3, 2)]
    start_all(to_pr)

    low_half = lax.broadcasted_iota(jnp.int32, (HEAD_DIM, 128), 1) < HEAD_DIM
    for p in range(PAIRS):
        both = lax.dot_general(tile(p), tile(p), (((0,), (0,)), ((), ())), preferred_element_type=F32)
        packed = jnp.where(low_half, both[0:HEAD_DIM], both[HEAD_DIM:])
        gp[:, p] = packed.reshape(NY, BLK, 128)

    rows = pl.ds(pl.multiple_of(y * BLK, BLK), BLK)
    wait_all(to_pr)
    pre = (pp[y] + pr[0]) + (pr[1] + pr[2])
    qm2 = MOMENT_DECAY * qm_ref[rows, :] + (1.0 - MOMENT_DECAY) * pre[:, :QN]
    km2 = MOMENT_DECAY * km_ref[rows, :] + (1.0 - MOMENT_DECAY) * pre[:, QN:]
    qw, kw = qw_ref[rows, :], kw_ref[rows, :]
    here = (y * NX + x) * NT + t
    plane[here] = jnp.concatenate(
        [lane_sums(v * v) for v in (qw, qm2, kw, km2)] + [jnp.zeros((4, 128), F32)], axis=0
    )
    mbuf[y, :, :QN] = qm2
    mbuf[y, :, QN:] = km2

    def slot_from(dy, dx, dt):
        return (y_of[(NY - dy) % NY] * NX + x_of[(NX - dx) % NX]) * NT + lax.rem(t + dt, NT)

    to_plane = [
        net.copy(
            plane.at[here], plane.at[here], {Y: y_of[dy], X: x_of[dx], T: lax.rem(t + dt, NT)},
            plane.at[slot_from(dy, dx, dt)],
        )
        for dy, dx, dt in others
    ]
    start_all(to_plane)
    to_m = [net.copy(mbuf.at[y], mbuf.at[y], {Y: y_of[d]}, mbuf.at[y_of[NY - d]]) for d in (1, 3, 2)]
    start_all(to_m)
    to_gr = [net.copy(gp.at[y_of[d]], gr.at[d - 1], {Y: y_of[d]}) for d in (1, 3, 2)]
    start_all(to_gr)
    wait_all(to_plane)
    total = plane[0]
    for i in range(1, NY * NX * NT):
        total = total + plane[i]
    zed[z] = total
    to_zed = [net.copy(zed.at[z], zed.at[z], {Z: z_of[d]}, zed.at[z_of[NZ - d]]) for d in (4, 3, 5, 2, 6, 1, 7)]
    start_all(to_zed)
    wait_all(to_zed)
    total = zed[0]
    for i in range(1, NZ):
        total = total + zed[i]
    total = jnp.sum(total, axis=1, keepdims=True)
    q_rate = LEARN_RATE * (jnp.sqrt(total[0:1]) / jnp.sqrt(total[1:2] + EPSILON))
    k_rate = LEARN_RATE * (jnp.sqrt(total[2:3]) / jnp.sqrt(total[3:4] + EPSILON))

    qcopy_ref[z, x, y] = (qw - q_rate * qm2).astype(BF16)
    kcopy_ref[z, x, y] = (kw - k_rate * km2).astype(BF16)

    def a_of(zi, xi, yi):
        return [qcopy_ref.at[zi, xi, yi, :, 0:WA]]

    def b_of(zi, xi, yi):
        return [qcopy_ref.at[zi, xi, yi, :, WA : WA + WB]]

    def c_of(zi, xi, yi):
        return [qcopy_ref.at[zi, xi, yi, :, WA + WB :], kcopy_ref.at[zi, xi, yi]]

    def spread(of, own, dev, source):
        return [net.copy(a, a, dev, b) for a, b in zip(of(*own), of(*source))]

    whole = slice(None)
    to_a, to_bz, to_cz, to_by, to_cx = [], [], [], [], []
    for dy, dx in spots[1:]:
        to_a += spread(a_of, (z, x, y), {Y: y_of[dy], X: x_of[dx]}, (z, x_of[(NX - dx) % NX], y_of[(NY - dy) % NY]))
    for d in (4, 3, 5, 2, 6, 1, 7):
        to_bz += spread(b_of, (z, x, y), {Z: z_of[d]}, (z_of[NZ - d], x, y))
        to_cz += spread(c_of, (z, x, y), {Z: z_of[d]}, (z_of[NZ - d], x, y))
    for d in (2, 1, 3):
        to_by += spread(b_of, (whole, x, y), {Y: y_of[d]}, (whole, x, y_of[NY - d]))
        to_cx += spread(c_of, (whole, x, y), {X: x_of[d]}, (whole, x_of[NX - d], y))
    ring_a = RingGather(net, Z, NZ, lambda c, h: a_of(c, pl.ds(2 * h, 2), whole))
    ring_b = RingGather(net, X, NX, lambda c, h: b_of(pl.ds(4 * h, 4), c, whole))
    ring_c = RingGather(net, Y, NY, lambda c, h: c_of(pl.ds(4 * h, 4), whole, c))

    start_all(to_a)
    start_all(to_bz)
    start_all(to_cz)
    wait_all(to_a)
    ring_a.send(0)
    ring_a.send(1)
    wait_all(to_bz)
    start_all(to_by)
    wait_all(to_cz)
    start_all(to_cx)

    wait_all(to_m)
    for yy in range(NY):
        at = slice(BLK * yy, BLK * (yy + 1))
        m = mbuf[yy, :, :QN]
        qm2_ref[at, :] = m
        qstep_ref[at, :] = q_rate * m
        qnext_ref[at, :] = qw_ref[at, :] - q_rate * m
        m = mbuf[yy, :, QN:]
        km2_ref[at, :] = m
        kstep_ref[at, :] = k_rate * m
        knext_ref[at, :] = kw_ref[at, :] - k_rate * m
    wait_all(to_gr)
    gfin[y] = (gp[y] + gr[0]) + (gr[1] + gr[2])
    to_gfin = [net.copy(gfin.at[y], gfin.at[y], {Y: y_of[d]}, gfin.at[y_of[NY - d]]) for d in (1, 3, 2)]

    ring_a.send(2)
    wait_all(to_by)
    ring_b.send(0)
    ring_b.send(1)
    ring_a.send(3)
    wait_all(to_cx)
    ring_c.send(0)
    ring_c.send(1)
    start_all(to_gfin)
    ring_a.send(4)
    ring_a.send(5)
    ring_b.send(2)
    ring_c.send(2)
    ring_a.send(6)

    wait_all(to_gfin)
    for p in range(PAIRS):
        source, target, h = (qs_ref, qs2_ref, 2 * p) if p < QPAIRS else (ks_ref, ks2_ref, 2 * (p - QPAIRS))
        gram = gfin[:, p].reshape(HEAD_DIM, 128) * ((1.0 - STAT_DECAY) / D)
        target[h] = STAT_DECAY * source[h] + gram[:, :HEAD_DIM]
        target[h + 1] = STAT_DECAY * source[h + 1] + gram[:, HEAD_DIM:]

    ring_b.finish()
    ring_c.finish()
    ring_a.finish()
    net.drain()


def shards(*args):
    space = pl.BlockSpec(memory_space=pltpu.VMEM)
    vm, dma = pltpu.VMEM, pltpu.SemaphoreType.DMA
    shape = jax.ShapeDtypeStruct
    blocks = (NZ, NX, NY, BLK)
    outs = pl.pallas_call(
        step_kernel,
        out_shape=(
            shape((64, QN), F32), shape((64, KN), F32),
            shape((64, QN), F32), shape((64, KN), F32),
            shape((*blocks, QN), BF16), shape((*blocks, KN), BF16),
            shape((64, QN), F32), shape((64, KN), F32),
            shape((16, 64, 64), F32), shape((4, 64, 64), F32),
        ),
        in_specs=[space] * 13,
        out_specs=[space] * 10,
        scratch_shapes=[
            vm((NY, NX, NZ, BLK, WA), F32),
            vm((NY, NX, NZ, BLK, WB), F32),
            vm((NY, NX, NZ, BLK, WC), F32),
            vm((2, 7, 2, NX, BLK, WA), F32),
            vm((2, 3, 2, NZ, BLK, WB), F32),
            vm((2, 3, 2, NZ, BLK, WC), F32),
            vm((15, BLK, WA), F32),
            vm((3, NZ, BLK, WB), F32),
            vm((3, NZ, BLK, WC), F32),
            vm((7, BLK, WB), F32),
            vm((7, BLK, WC), F32),
            vm((NX, NZ, BLK, QN + KN), BF16),
            vm((PAIRS, 128, 128), BF16),
            vm((NY, BLK, QN + KN), F32),
            vm((3, BLK, QN + KN), F32),
            vm((NY, BLK, QN + KN), F32),
            vm((NY, PAIRS, BLK, 128), F32),
            vm((3, PAIRS, BLK, 128), F32),
            vm((NY, PAIRS, BLK, 128), F32),
            vm((NY * NX * NT, 8, 128), F32),
            vm((NZ, 8, 128), F32),
            dma((COPIES,)),
            dma((COPIES,)),
        ],
        compiler_params=pltpu.CompilerParams(
            collective_id=0, has_side_effects=True, vmem_limit_bytes=62 * 2**20
        ),
        name="step",
    )(*args)
    outs = list(outs)
    outs[4] = outs[4].reshape(D, QN)
    outs[5] = outs[5].reshape(D, KN)
    return tuple(outs)


def solution(mesh):
    split = Mesh(mesh.devices.reshape(NZ, NX, NY, NT), (Z, X, Y, T))
    row = P(FS, T)
    head = P(T, None, None)
    whole = P(None, T)
    tok = P(FS_REP, T)
    return jax.shard_map(
        shards, mesh=split,
        in_specs=(P(FS_REP, None), tok, tok, row, row, row, row, P(FS, None), P(FS, None), head, head, head, head),
        out_specs=(row, row, row, row, whole, whole, row, row, head, head),
        check_vma=False,
    )
```

```python
import jax
import jax.numpy as jnp
from jax import lax
from jax.experimental import pallas as pl
from jax.experimental.pallas import tpu as pltpu
from jax.sharding import Mesh
from jax.sharding import PartitionSpec as P

D = 2048
HEAD_DIM = 64
NZ, NX, NY, NT = 8, 4, 4, 2
Z, X, Y, T = "fs_0", "fs_1", "rep", "tp"
FS = (Z, X)
FS_REP = (Z, X, Y)
MOMENT_DECAY = 0.8
STAT_DECAY = 0.5
LEARN_RATE = 0.1
EPSILON = 1e-06
MESH = pl.DeviceIdType.MESH
QN, KN = 1024, 256
WA, WB, WC = 512, 384, 384
WP = 640
BLK = 16
PAIRS = 10
QPAIRS = 8
COPIES = 256
F32, BF16 = jnp.float32, jnp.bfloat16


class Net:
    def __init__(self, send_sem, recv_sem):
        self.send_sem, self.recv_sem, self.used, self.sent = send_sem, recv_sem, 0, []

    def copy(self, src, dst, dev, landing=None):
        k = self.used
        self.used += 1
        copies = [
            pltpu.make_async_remote_copy(
                src_ref=a, dst_ref=b, send_sem=self.send_sem.at[k], recv_sem=self.recv_sem.at[k],
                device_id=dev, device_id_type=MESH,
            )
            for a, b in ((src, dst), (dst, dst) if landing is None else (landing, landing))
        ]
        return Copy(self, *copies)

    def drain(self):
        for copy in self.sent:
            copy.wait_send()


class Copy:
    def __init__(self, net, out, into):
        self.net, self.out, self.into = net, out, into

    def start(self):
        self.out.start()
        self.net.sent.append(self.out)

    def wait(self):
        self.into.wait_recv()


def start_all(copies):
    for copy in copies:
        copy.start()


def wait_all(copies):
    for copy in copies:
        copy.wait()


class Ring:
    def __init__(self, axis, n):
        self.n, self.me = n, lax.axis_index(axis)
        self.copies = {}
        self.device = [{axis: self.place(way, 1)} for way in range(2)]

    def place(self, way, dist):
        return lax.rem(self.me + (dist if way == 0 else self.n - dist), self.n)


class RingSum(Ring):
    def __init__(self, net, axis, n, region, recv, add):
        super().__init__(axis, n)
        self.recv, self.add = recv, add
        self.slots = [(n // 2, 0, None)]
        for k in range(1, n // 2):
            self.slots.append((n // 2 - k, 1, 2 * k - 3 if k >= 2 else None))
            self.slots.append((n // 2 - k, 0, 2 * k - 2))
        for way in range(2):
            for j, (dist, half, _) in enumerate(self.slots):
                self.copies[way, j] = net.copy(
                    region(self.place(way, dist), half ^ way), recv.at[way, j], self.device[way]
                )

    def send(self, j):
        for way in range(2):
            dist, half, source = self.slots[j]
            if source is not None:
                self.copies[way, source].wait()
                self.add(self.place(way, dist), half ^ way, self.recv.at[way, source])
            self.copies[way, j].start()

    def finish(self):
        for j in (self.n - 3, self.n - 2):
            for way in range(2):
                self.copies[way, j].wait()
                self.add(self.me, self.slots[j][1] ^ way, self.recv.at[way, j])


class RingGather(Ring):
    def __init__(self, net, axis, n, regions):
        super().__init__(axis, n)
        slots = [(j // 2, j % 2) for j in range(n - 1)]
        for way in range(2):
            for j, (k, half) in enumerate(slots):
                held = regions(self.place(1 - way, k), half ^ way)
                coming = regions(self.place(1 - way, k + 1), half ^ way)
                self.copies[way, j] = [
                    net.copy(a, a, self.device[way], b) for a, b in zip(held, coming)
                ]

    def send(self, j):
        for way in range(2):
            if j >= 2:
                wait_all(self.copies[way, j - 2])
            start_all(self.copies[way, j])

    def finish(self):
        for j in (self.n - 3, self.n - 2):
            for way in range(2):
                wait_all(self.copies[way, j])


def lane_sums(value):
    total = value[:, 0:128]
    for i in range(1, value.shape[1] // 128):
        total = total + value[:, 128 * i : 128 * (i + 1)]
    return jnp.sum(total, axis=0, keepdims=True)


def step_kernel(
    x_hbm, qc_hbm, kc_hbm, qw_hbm, kw_hbm, qm_hbm, km_hbm, ql_hbm, kl_hbm, qr_hbm, kr_hbm, qs_hbm, ks_hbm,
    qstep_ref, kstep_ref, qnext_ref, knext_ref, qcopy_ref, kcopy_ref, qm2_ref, km2_ref, qs2_ref, ks2_ref,
    ga, gb, gc, ra, rb, rc, pa, b1, c1, b2, c2,
    gath, roots, pp, pr, mbuf, gp, gr, gfin, plane, zed,
    x_ref, qc_ref, kc_ref, qw_ref, kw_ref, qm_ref, km_ref, ql_ref, kl_ref, qr_ref, kr_ref, qs_ref, ks_ref,
    send_sem, recv_sem, load_sem,
):
    z, x, y, t = (lax.axis_index(a) for a in (Z, X, Y, T))
    z_of = [lax.rem(z + d, NZ) for d in range(NZ)]
    x_of = [lax.rem(x + d, NX) for d in range(NX)]
    y_of = [lax.rem(y + d, NY) for d in range(NY)]
    spots = [(dy, dx) for dy in range(NY) for dx in range(NX)]
    others = [(dy, dx, dt) for dy, dx in spots for dt in range(NT) if dy or dx or dt]
    net = Net(send_sem, recv_sem)

    peers = [{Z: z_of[d]} for d in range(1, NZ)] + [
        {Y: y_of[dy], X: x_of[dx], T: lax.rem(t + dt, NT)} for dy, dx, dt in others
    ]
    barrier = pltpu.get_barrier_semaphore()
    for dev in peers:
        pl.semaphore_signal(barrier, inc=1, device_id=dev, device_id_type=MESH)

    l_at = pl.ds(pl.multiple_of(y * 512, 512), 512)
    loads = [(qc_hbm, qc_ref)]
    loads += [(x_hbm.at[:, 512 * i : 512 * (i + 1)], x_ref.at[i]) for i in range(NY)]
    loads += [(kc_hbm, kc_ref), (qr_hbm, qr_ref), (kr_hbm, kr_ref)]
    loads += [(ql_hbm.at[:, l_at], ql_ref), (kl_hbm.at[:, l_at], kl_ref)]
    loads += [(qw_hbm, qw_ref), (kw_hbm, kw_ref), (qm_hbm, qm_ref), (km_hbm, km_ref)]
    loads += [(qs_hbm, qs_ref), (ks_hbm, ks_ref)]
    loads = [pltpu.make_async_copy(a, b, load_sem.at[i]) for i, (a, b) in enumerate(loads)]
    start_all(loads)

    def product(rows, cot, low, width):
        return lax.dot_general(
            rows, cot[:, low : low + width], (((0,), (0,)), ((), ())), preferred_element_type=F32
        )

    def add_a(chunk, half, recv):
        for y2 in range(2):
            def body(x2, _):
                at = (2 * half + y2, x2, chunk)
                ga[at] = ga[at] + recv[y2, x2]
                return 0
            lax.fori_loop(0, NX, body, 0)

    def add_b(chunk, half, recv):
        for y2 in range(2):
            def body(z2, _):
                at = (2 * half + y2, chunk, z2)
                gb[at] = gb[at] + recv[y2, z2]
                return 0
            lax.fori_loop(0, NZ, body, 0)

    def add_c(chunk, half, recv):
        for x2 in range(2):
            def body(z2, _):
                at = (chunk, 2 * half + x2, z2)
                gc[at] = gc[at] + recv[x2, z2]
                return 0
            lax.fori_loop(0, NZ, body, 0)

    ring_a = RingSum(net, Z, NZ, lambda c, h: ga.at[pl.ds(2 * h, 2), :, c], ra, add_a)
    ring_b = RingSum(net, X, NX, lambda c, h: gb.at[pl.ds(2 * h, 2), c], rb, add_b)
    ring_c = RingSum(net, Y, NY, lambda c, h: gc.at[c, pl.ds(2 * h, 2)], rc, add_c)

    def make_b(chunk):
        at = pl.ds(pl.multiple_of(chunk * 128, 128), 128)
        rows = jnp.concatenate([x_ref[i, :, at] for i in range(NY)], axis=1)
        gb[:, chunk] = product(rows, qc_ref, WA, WB).reshape(NY, NZ, BLK, WB)

    def make_c(chunk):
        rows = x_ref[chunk]
        gc[chunk, :, :, :, 0:128] = product(rows, qc_ref, WA + WB, 128).reshape(NX, NZ, BLK, 128)
        gc[chunk, :, :, :, 128:WC] = product(rows, kc_ref, 0, KN).reshape(NX, NZ, BLK, KN)

    loads[0].wait()
    for i in range(NY):
        loads[1 + i].wait()
        ga[i] = product(x_ref[i], qc_ref, 0, WA).reshape(NX, NZ, BLK, WA)
    pl.semaphore_wait(barrier, len(peers))
    ring_a.send(0)
    ring_a.send(1)
    make_b(x_of[2])
    ring_b.send(0)
    for load in loads[1 + NY :]:
        load.wait()
    make_c(y_of[2])
    ring_c.send(0)
    make_b(x_of[1])
    make_b(x_of[3])
    ring_b.send(1)
    make_c(y_of[1])
    make_c(y_of[3])
    ring_c.send(1)
    ring_a.send(2)
    make_b(x_of[0])
    make_c(y_of[0])

    roots[...] = jnp.zeros_like(roots)
    for p in range(PAIRS):
        ref, h = (qr_ref, 2 * p) if p < QPAIRS else (kr_ref, 2 * (p - QPAIRS))
        roots[p, 0:HEAD_DIM, 0:HEAD_DIM] = ref[h]
        roots[p, HEAD_DIM : 2 * HEAD_DIM, HEAD_DIM : 2 * HEAD_DIM] = ref[h + 1]

    ring_a.send(3)
    ring_b.send(2)
    ring_c.send(2)
    ring_a.send(4)
    ring_a.send(5)
    ring_a.send(6)

    ring_c.finish()
    to_c1 = [net.copy(gc.at[y, x_of[d]], c1.at[d - 1], {X: x_of[d]}) for d in (1, 3, 2)]
    start_all(to_c1)
    ring_b.finish()
    to_b1 = [net.copy(gb.at[y_of[d], x], b1.at[d - 1], {Y: y_of[d]}) for d in (1, 3, 2)]
    start_all(to_b1)

    wait_all(to_c1)
    def sum_c(zz, _):
        gc[y, x, zz] = (gc[y, x, zz] + c1[0, zz]) + (c1[1, zz] + c1[2, zz])
        return 0
    lax.fori_loop(0, NZ, sum_c, 0)
    to_c2 = [net.copy(gc.at[y, x, z_of[d]], c2.at[d - 1], {Z: z_of[d]}) for d in range(1, NZ)]
    start_all(to_c2)

    ring_a.finish()
    to_pa = [
        net.copy(ga.at[y_of[dy], x_of[dx], z], pa.at[i], {Y: y_of[dy], X: x_of[dx]})
        for i, (dy, dx) in enumerate(spots[1:])
    ]
    start_all(to_pa)

    wait_all(to_b1)
    def sum_b(zz, _):
        gb[y, x, zz] = (gb[y, x, zz] + b1[0, zz]) + (b1[1, zz] + b1[2, zz])
        return 0
    lax.fori_loop(0, NZ, sum_b, 0)
    to_b2 = [net.copy(gb.at[y, x, z_of[d]], b2.at[d - 1], {Z: z_of[d]}) for d in range(1, NZ)]
    start_all(to_b2)

    mine = gath.at[x, z]

    def settle(own, arrived, low, width):
        total = own
        for d in range(arrived.shape[0]):
            total = total + arrived[d]
        mine[:, low : low + width] = total.astype(BF16)

    wait_all(to_c2)
    settle(gc[y, x, z], c2, WA + WB, WC)
    wait_all(to_pa)
    settle(ga[y, x, z], pa, 0, WA)
    wait_all(to_b2)
    settle(gb[y, x, z], b2, WA, WB)

    p_x = [net.copy(gath.at[x, z, :, 0:WP], gath.at[x, z, :, 0:WP], {X: x_of[d]}, gath.at[x_of[NX - d], z, :, 0:WP]) for d in (1, 3, 2)]
    start_all(p_x)
    q_z = [net.copy(gath.at[x, z, :, WP:], gath.at[x, z, :, WP:], {Z: z_of[d]}, gath.at[x, z_of[NZ - d], :, WP:]) for d in (4, 3, 5, 2, 6, 1, 7)]
    start_all(q_z)
    ring_p = RingGather(net, Z, NZ, lambda c, h: [gath.at[pl.ds(2 * h, 2), c, :, 0:WP]])
    wait_all(p_x)
    ring_p.send(0)
    ring_p.send(1)
    wait_all(q_z)
    q_x = [net.copy(gath.at[x, :, :, WP:], gath.at[x, :, :, WP:], {X: x_of[d]}, gath.at[x_of[NX - d], :, :, WP:]) for d in (1, 3, 2)]
    start_all(q_x)
    for j in range(2, NZ - 1):
        ring_p.send(j)

    def tile(p):
        return gath[:, :, :, 128 * p : 128 * (p + 1)].reshape(NX * NZ * BLK, 128)

    def precondition(p):
        right = jnp.dot(tile(p), roots[p], preferred_element_type=F32).astype(BF16)
        left = ql_ref if p < QPAIRS else kl_ref
        part = jnp.dot(left[...], right, preferred_element_type=F32)
        pp[:, :, 128 * p : 128 * (p + 1)] = part.reshape(NY, BLK, 128)

    wait_all(q_x)
    for p in range(WP // 128, PAIRS):
        precondition(p)
    ring_p.finish()
    for p in range(WP // 128):
        precondition(p)

    to_pr = [net.copy(pp.at[y_of[d]], pr.at[d - 1], {Y: y_of[d]}) for d in (1, 3, 2)]
    start_all(to_pr)

    low_half = lax.broadcasted_iota(jnp.int32, (HEAD_DIM, 128), 1) < HEAD_DIM
    for p in range(PAIRS):
        both = lax.dot_general(tile(p), tile(p), (((0,), (0,)), ((), ())), preferred_element_type=F32)
        packed = jnp.where(low_half, both[0:HEAD_DIM], both[HEAD_DIM:])
        gp[:, p] = packed.reshape(NY, BLK, 128)

    rows = pl.ds(pl.multiple_of(y * BLK, BLK), BLK)
    wait_all(to_pr)
    pre = (pp[y] + pr[0]) + (pr[1] + pr[2])
    qm2 = MOMENT_DECAY * qm_ref[rows, :] + (1.0 - MOMENT_DECAY) * pre[:, :QN]
    km2 = MOMENT_DECAY * km_ref[rows, :] + (1.0 - MOMENT_DECAY) * pre[:, QN:]
    qw, kw = qw_ref[rows, :], kw_ref[rows, :]
    here = (y * NX + x) * NT + t
    plane[here] = jnp.concatenate(
        [lane_sums(v * v) for v in (qw, qm2, kw, km2)] + [jnp.zeros((4, 128), F32)], axis=0
    )
    mbuf[y, :, :QN] = qm2
    mbuf[y, :, QN:] = km2

    def slot_from(dy, dx, dt):
        return (y_of[(NY - dy) % NY] * NX + x_of[(NX - dx) % NX]) * NT + lax.rem(t + dt, NT)

    to_plane = [
        net.copy(
            plane.at[here], plane.at[here], {Y: y_of[dy], X: x_of[dx], T: lax.rem(t + dt, NT)},
            plane.at[slot_from(dy, dx, dt)],
        )
        for dy, dx, dt in others
    ]
    start_all(to_plane)
    to_m = [net.copy(mbuf.at[y], mbuf.at[y], {Y: y_of[d]}, mbuf.at[y_of[NY - d]]) for d in (1, 3, 2)]
    start_all(to_m)
    to_gr = [net.copy(gp.at[y_of[d]], gr.at[d - 1], {Y: y_of[d]}) for d in (1, 3, 2)]
    start_all(to_gr)
    wait_all(to_plane)
    total = plane[0]
    for i in range(1, NY * NX * NT):
        total = total + plane[i]
    zed[z] = total
    to_zed = [net.copy(zed.at[z], zed.at[z], {Z: z_of[d]}, zed.at[z_of[NZ - d]]) for d in (4, 3, 5, 2, 6, 1, 7)]
    start_all(to_zed)
    wait_all(to_zed)
    total = zed[0]
    for i in range(1, NZ):
        total = total + zed[i]
    total = jnp.sum(total, axis=1, keepdims=True)
    q_rate = LEARN_RATE * (jnp.sqrt(total[0:1]) / jnp.sqrt(total[1:2] + EPSILON))
    k_rate = LEARN_RATE * (jnp.sqrt(total[2:3]) / jnp.sqrt(total[3:4] + EPSILON))

    qcopy_ref[z, x, y] = (qw - q_rate * qm2).astype(BF16)
    kcopy_ref[z, x, y] = (kw - k_rate * km2).astype(BF16)

    def a_of(zi, xi, yi):
        return [qcopy_ref.at[zi, xi, yi, :, 0:WA]]

    def b_of(zi, xi, yi):
        return [qcopy_ref.at[zi, xi, yi, :, WA : WA + WB]]

    def c_of(zi, xi, yi):
        return [qcopy_ref.at[zi, xi, yi, :, WA + WB :], kcopy_ref.at[zi, xi, yi]]

    def spread(of, own, dev, source):
        return [net.copy(a, a, dev, b) for a, b in zip(of(*own), of(*source))]

    whole = slice(None)
    to_a, to_bz, to_cz, to_by, to_cx = [], [], [], [], []
    for dy, dx in spots[1:]:
        to_a += spread(a_of, (z, x, y), {Y: y_of[dy], X: x_of[dx]}, (z, x_of[(NX - dx) % NX], y_of[(NY - dy) % NY]))
    for d in (4, 3, 5, 2, 6, 1, 7):
        to_bz += spread(b_of, (z, x, y), {Z: z_of[d]}, (z_of[NZ - d], x, y))
        to_cz += spread(c_of, (z, x, y), {Z: z_of[d]}, (z_of[NZ - d], x, y))
    for d in (2, 1, 3):
        to_by += spread(b_of, (whole, x, y), {Y: y_of[d]}, (whole, x, y_of[NY - d]))
        to_cx += spread(c_of, (whole, x, y), {X: x_of[d]}, (whole, x_of[NX - d], y))
    ring_a = RingGather(net, Z, NZ, lambda c, h: a_of(c, pl.ds(2 * h, 2), whole))
    ring_b = RingGather(net, X, NX, lambda c, h: b_of(pl.ds(4 * h, 4), c, whole))
    ring_c = RingGather(net, Y, NY, lambda c, h: c_of(pl.ds(4 * h, 4), whole, c))

    start_all(to_a)
    start_all(to_bz)
    start_all(to_cz)
    wait_all(to_a)
    ring_a.send(0)
    ring_a.send(1)
    wait_all(to_bz)
    start_all(to_by)
    wait_all(to_cz)
    start_all(to_cx)

    wait_all(to_m)
    for yy in range(NY):
        at = slice(BLK * yy, BLK * (yy + 1))
        m = mbuf[yy, :, :QN]
        qm2_ref[at, :] = m
        qstep_ref[at, :] = q_rate * m
        qnext_ref[at, :] = qw_ref[at, :] - q_rate * m
        m = mbuf[yy, :, QN:]
        km2_ref[at, :] = m
        kstep_ref[at, :] = k_rate * m
        knext_ref[at, :] = kw_ref[at, :] - k_rate * m
    wait_all(to_gr)
    gfin[y] = (gp[y] + gr[0]) + (gr[1] + gr[2])
    to_gfin = [net.copy(gfin.at[y], gfin.at[y], {Y: y_of[d]}, gfin.at[y_of[NY - d]]) for d in (1, 3, 2)]

    ring_a.send(2)
    wait_all(to_by)
    ring_b.send(0)
    ring_b.send(1)
    ring_a.send(3)
    wait_all(to_cx)
    ring_c.send(0)
    ring_c.send(1)
    start_all(to_gfin)
    ring_a.send(4)
    ring_a.send(5)
    ring_b.send(2)
    ring_c.send(2)
    ring_a.send(6)

    wait_all(to_gfin)
    for p in range(PAIRS):
        source, target, h = (qs_ref, qs2_ref, 2 * p) if p < QPAIRS else (ks_ref, ks2_ref, 2 * (p - QPAIRS))
        gram = gfin[:, p].reshape(HEAD_DIM, 128) * ((1.0 - STAT_DECAY) / D)
        target[h] = STAT_DECAY * source[h] + gram[:, :HEAD_DIM]
        target[h + 1] = STAT_DECAY * source[h + 1] + gram[:, HEAD_DIM:]

    ring_b.finish()
    ring_c.finish()
    ring_a.finish()
    net.drain()


def write_kernel(*refs):
    n = len(refs) // 2
    sem = refs[-1]
    copies = [pltpu.make_async_copy(refs[i], refs[n + i], sem.at[i]) for i in range(n)]
    start_all(copies)
    wait_all(copies)


def shards(*args):
    hbm = pl.BlockSpec(memory_space=pltpu.HBM)
    space = pl.BlockSpec(memory_space=pltpu.VMEM)
    vm, dma = pltpu.VMEM, pltpu.SemaphoreType.DMA
    blocks = (NZ, NX, NY, BLK)
    outs = (
        ((64, QN), F32), ((64, KN), F32),
        ((64, QN), F32), ((64, KN), F32),
        ((*blocks, QN), BF16), ((*blocks, KN), BF16),
        ((64, QN), F32), ((64, KN), F32),
        ((16, 64, 64), F32), ((4, 64, 64), F32),
    )
    results = pl.pallas_call(
        step_kernel,
        out_shape=tuple(vm(*o) for o in outs),
        in_specs=[hbm] * 13,
        out_specs=[space] * 10,
        scratch_shapes=[
            vm((NY, NX, NZ, BLK, WA), F32),
            vm((NY, NX, NZ, BLK, WB), F32),
            vm((NY, NX, NZ, BLK, WC), F32),
            vm((2, 7, 2, NX, BLK, WA), F32),
            vm((2, 3, 2, NZ, BLK, WB), F32),
            vm((2, 3, 2, NZ, BLK, WC), F32),
            vm((15, BLK, WA), F32),
            vm((3, NZ, BLK, WB), F32),
            vm((3, NZ, BLK, WC), F32),
            vm((7, BLK, WB), F32),
            vm((7, BLK, WC), F32),
            vm((NX, NZ, BLK, QN + KN), BF16),
            vm((PAIRS, 128, 128), BF16),
            vm((NY, BLK, QN + KN), F32),
            vm((3, BLK, QN + KN), F32),
            vm((NY, BLK, QN + KN), F32),
            vm((NY, PAIRS, BLK, 128), F32),
            vm((3, PAIRS, BLK, 128), F32),
            vm((NY, PAIRS, BLK, 128), F32),
            vm((NY * NX * NT, 8, 128), F32),
            vm((NZ, 8, 128), F32),
            vm((NY, 1024, 512), BF16), vm((1024, QN), BF16), vm((1024, KN), BF16),
            vm((64, QN), F32), vm((64, KN), F32), vm((64, QN), F32), vm((64, KN), F32),
            vm((64, 512), BF16), vm((64, 512), BF16),
            vm((16, 64, 64), BF16), vm((4, 64, 64), BF16), vm((16, 64, 64), F32), vm((4, 64, 64), F32),
            dma((COPIES,)),
            dma((COPIES,)),
            dma((16,)),
        ],
        compiler_params=pltpu.CompilerParams(
            collective_id=0, has_side_effects=True, vmem_limit_bytes=46 * 2**20
        ),
        name="step",
    )(*(pltpu.with_memory_space_constraint(a, pltpu.HBM) for a in args))
    written = list(pl.pallas_call(
        write_kernel,
        out_shape=tuple(jax.ShapeDtypeStruct(*o) for o in outs),
        in_specs=[space] * 10,
        out_specs=[hbm] * 10,
        scratch_shapes=[dma((10,))],
        compiler_params=pltpu.CompilerParams(vmem_limit_bytes=2**20),
        name="write",
    )(*(pltpu.with_memory_space_constraint(r, pltpu.VMEM) for r in results)))
    written[4] = written[4].reshape(D, QN)
    written[5] = written[5].reshape(D, KN)
    return tuple(written)


def solution(mesh):
    split = Mesh(mesh.devices.reshape(NZ, NX, NY, NT), (Z, X, Y, T))
    row = P(FS, T)
    head = P(T, None, None)
    whole = P(None, T)
    tok = P(FS_REP, T)
    return jax.shard_map(
        shards, mesh=split,
        in_specs=(P(FS_REP, None), tok, tok, row, row, row, row, P(FS, None), P(FS, None), head, head, head, head),
        out_specs=(row, row, row, row, whole, whole, row, row, head, head),
        check_vma=False,
    )
```

```python
import jax
import jax.numpy as jnp
from jax import lax
from jax.experimental import pallas as pl
from jax.experimental.pallas import tpu as pltpu
from jax.sharding import Mesh
from jax.sharding import PartitionSpec as P

D = 2048
HEAD_DIM = 64
NZ, NX, NY, NT = 8, 4, 4, 2
Z, X, Y, T = "fs_0", "fs_1", "rep", "tp"
FS = (Z, X)
FS_REP = (Z, X, Y)
MOMENT_DECAY = 0.8
STAT_DECAY = 0.5
LEARN_RATE = 0.1
EPSILON = 1e-06
MESH = pl.DeviceIdType.MESH
QN, KN = 1024, 256
WA, WB, WC = 512, 384, 384
WP = 256
BLK = 16
PAIRS = 10
QPAIRS = 8
COPIES = 288
NEAR = (1, 7, 2, 6, 3, 5, 4)
F32, BF16 = jnp.float32, jnp.bfloat16


class Net:
    def __init__(self, send_sem, recv_sem):
        self.send_sem, self.recv_sem, self.used, self.sent = send_sem, recv_sem, 0, []

    def copy(self, src, dst, dev, landing=None):
        k = self.used
        self.used += 1
        copies = [
            pltpu.make_async_remote_copy(
                src_ref=a, dst_ref=b, send_sem=self.send_sem.at[k], recv_sem=self.recv_sem.at[k],
                device_id=dev, device_id_type=MESH,
            )
            for a, b in ((src, dst), (dst, dst) if landing is None else (landing, landing))
        ]
        return Copy(self, *copies)

    def drain(self):
        for copy in self.sent:
            copy.wait_send()


class Copy:
    def __init__(self, net, out, into):
        self.net, self.out, self.into = net, out, into

    def start(self):
        self.out.start()
        self.net.sent.append(self.out)

    def wait(self):
        self.into.wait_recv()


def start_all(copies):
    for copy in copies:
        copy.start()


def wait_all(copies):
    for copy in copies:
        copy.wait()


class Ring:
    def __init__(self, axis, n):
        self.n, self.me = n, lax.axis_index(axis)
        self.copies = {}
        self.device = [{axis: self.place(way, 1)} for way in range(2)]

    def place(self, way, dist):
        return lax.rem(self.me + (dist if way == 0 else self.n - dist), self.n)


class RingSum(Ring):
    def __init__(self, net, axis, n, region, recv, add):
        super().__init__(axis, n)
        self.recv, self.add = recv, add
        self.slots = [(n // 2, 0, None)]
        for k in range(1, n // 2):
            self.slots.append((n // 2 - k, 1, 2 * k - 3 if k >= 2 else None))
            self.slots.append((n // 2 - k, 0, 2 * k - 2))
        for way in range(2):
            for j, (dist, half, _) in enumerate(self.slots):
                self.copies[way, j] = net.copy(
                    region(self.place(way, dist), half ^ way), recv.at[way, j], self.device[way]
                )

    def send(self, j):
        for way in range(2):
            dist, half, source = self.slots[j]
            if source is not None:
                self.copies[way, source].wait()
                self.add(self.place(way, dist), half ^ way, self.recv.at[way, source])
            self.copies[way, j].start()

    def finish(self):
        for j in (self.n - 3, self.n - 2):
            for way in range(2):
                self.copies[way, j].wait()
                self.add(self.me, self.slots[j][1] ^ way, self.recv.at[way, j])


class RingGather(Ring):
    def __init__(self, net, axis, n, regions):
        super().__init__(axis, n)
        slots = [(j // 2, j % 2) for j in range(n - 1)]
        for way in range(2):
            for j, (k, half) in enumerate(slots):
                held = regions(self.place(1 - way, k), half ^ way)
                coming = regions(self.place(1 - way, k + 1), half ^ way)
                self.copies[way, j] = [
                    net.copy(a, a, self.device[way], b) for a, b in zip(held, coming)
                ]

    def send(self, j):
        for way in range(2):
            if j >= 2:
                wait_all(self.copies[way, j - 2])
            start_all(self.copies[way, j])

    def finish(self):
        for j in (self.n - 3, self.n - 2):
            for way in range(2):
                wait_all(self.copies[way, j])


def lane_sums(value):
    total = value[:, 0:128]
    for i in range(1, value.shape[1] // 128):
        total = total + value[:, 128 * i : 128 * (i + 1)]
    return jnp.sum(total, axis=0, keepdims=True)


def step_kernel(
    x_hbm, qc_hbm, kc_hbm, qw_hbm, kw_hbm, qm_hbm, km_hbm, ql_hbm, kl_hbm, qr_hbm, kr_hbm, qs_hbm, ks_hbm,
    qstep_ref, kstep_ref, qnext_ref, knext_ref, qcopy_ref, kcopy_ref, qm2_ref, km2_ref, qs2_ref, ks2_ref,
    ga, gb, gc, ra, rb, rc, pa, b1, c1, b2, c2,
    gath, roots, pp, pr, mbuf, gp, gr, gfin, plane, zed,
    x_ref, qc_ref, kc_ref, qw_ref, kw_ref, qm_ref, km_ref, ql_ref, kl_ref, qr_ref, kr_ref, qs_ref, ks_ref,
    send_sem, recv_sem, load_sem,
):
    z, x, y, t = (lax.axis_index(a) for a in (Z, X, Y, T))
    z_of = [lax.rem(z + d, NZ) for d in range(NZ)]
    x_of = [lax.rem(x + d, NX) for d in range(NX)]
    y_of = [lax.rem(y + d, NY) for d in range(NY)]
    spots = [(dy, dx) for dy in range(NY) for dx in range(NX)]
    spots.sort(key=lambda s: -min(s[0], NY - s[0]) - min(s[1], NX - s[1]))
    spots = [(0, 0)] + spots[:-1]
    others = [(dy, dx, dt) for dy, dx in spots for dt in range(NT) if dy or dx or dt]
    net = Net(send_sem, recv_sem)

    peers = [{Z: z_of[d]} for d in range(1, NZ)] + [
        {Y: y_of[dy], X: x_of[dx], T: lax.rem(t + dt, NT)} for dy, dx, dt in others
    ]
    barrier = pltpu.get_barrier_semaphore()
    for dev in peers:
        pl.semaphore_signal(barrier, inc=1, device_id=dev, device_id_type=MESH)

    l_at = pl.ds(pl.multiple_of(y * 512, 512), 512)
    loads = [(qc_hbm, qc_ref)]
    loads += [(x_hbm.at[:, 512 * i : 512 * (i + 1)], x_ref.at[i]) for i in range(NY)]
    loads += [(kc_hbm, kc_ref), (qr_hbm, qr_ref), (kr_hbm, kr_ref)]
    loads += [(ql_hbm.at[:, l_at], ql_ref), (kl_hbm.at[:, l_at], kl_ref)]
    loads += [(qw_hbm, qw_ref), (kw_hbm, kw_ref), (qm_hbm, qm_ref), (km_hbm, km_ref)]
    loads += [(qs_hbm, qs_ref), (ks_hbm, ks_ref)]
    loads = [pltpu.make_async_copy(a, b, load_sem.at[i]) for i, (a, b) in enumerate(loads)]
    start_all(loads)

    def product(rows, cot, low, width):
        return lax.dot_general(
            rows, cot[:, low : low + width], (((0,), (0,)), ((), ())), preferred_element_type=F32
        )

    def add_a(chunk, half, recv):
        for y2 in range(2):
            def body(x2, _):
                at = (2 * half + y2, x2, chunk)
                ga[at] = ga[at] + recv[y2, x2]
                return 0
            lax.fori_loop(0, NX, body, 0)

    def add_b(chunk, half, recv):
        for y2 in range(2):
            def body(z2, _):
                at = (2 * half + y2, chunk, z2)
                gb[at] = gb[at] + recv[y2, z2]
                return 0
            lax.fori_loop(0, NZ, body, 0)

    def add_c(chunk, half, recv):
        for x2 in range(2):
            def body(z2, _):
                at = (chunk, 2 * half + x2, z2)
                gc[at] = gc[at] + recv[x2, z2]
                return 0
            lax.fori_loop(0, NZ, body, 0)

    ring_a = RingSum(net, Z, NZ, lambda c, h: ga.at[pl.ds(2 * h, 2), :, c], ra, add_a)
    ring_b = RingSum(net, X, NX, lambda c, h: gb.at[pl.ds(2 * h, 2), c], rb, add_b)
    ring_c = RingSum(net, Y, NY, lambda c, h: gc.at[c, pl.ds(2 * h, 2)], rc, add_c)

    def make_b(chunk):
        at = pl.ds(pl.multiple_of(chunk * 128, 128), 128)
        rows = jnp.concatenate([x_ref[i, :, at] for i in range(NY)], axis=1)
        gb[:, chunk] = product(rows, qc_ref, WA, WB).reshape(NY, NZ, BLK, WB)

    def make_c(chunk):
        rows = x_ref[chunk]
        gc[chunk, :, :, :, 0:128] = product(rows, qc_ref, WA + WB, 128).reshape(NX, NZ, BLK, 128)
        gc[chunk, :, :, :, 128:WC] = product(rows, kc_ref, 0, KN).reshape(NX, NZ, BLK, KN)

    loads[0].wait()
    for i in range(NY):
        loads[1 + i].wait()
        ga[i] = product(x_ref[i], qc_ref, 0, WA).reshape(NX, NZ, BLK, WA)
    pl.semaphore_wait(barrier, len(peers))
    ring_a.send(0)
    ring_a.send(1)
    make_b(x_of[2])
    ring_b.send(0)
    for load in loads[1 + NY :]:
        load.wait()
    make_c(y_of[2])
    ring_c.send(0)
    make_b(x_of[1])
    make_b(x_of[3])
    ring_b.send(1)
    make_c(y_of[1])
    make_c(y_of[3])
    ring_c.send(1)
    ring_a.send(2)
    make_b(x_of[0])
    make_c(y_of[0])

    roots[...] = jnp.zeros_like(roots)
    for p in range(PAIRS):
        ref, h = (qr_ref, 2 * p) if p < QPAIRS else (kr_ref, 2 * (p - QPAIRS))
        roots[p, 0:HEAD_DIM, 0:HEAD_DIM] = ref[h]
        roots[p, HEAD_DIM : 2 * HEAD_DIM, HEAD_DIM : 2 * HEAD_DIM] = ref[h + 1]

    ring_a.send(3)
    ring_b.send(2)
    ring_c.send(2)
    ring_a.send(4)
    ring_a.send(5)
    ring_a.send(6)

    ring_c.finish()
    to_c1 = [net.copy(gc.at[y, x_of[d]], c1.at[d - 1], {X: x_of[d]}) for d in (1, 3, 2)]
    start_all(to_c1)
    ring_b.finish()
    to_b1 = [net.copy(gb.at[y_of[d], x], b1.at[d - 1], {Y: y_of[d]}) for d in (1, 3, 2)]
    start_all(to_b1)

    wait_all(to_c1)
    def sum_c(zz, _):
        gc[y, x, zz] = (gc[y, x, zz] + c1[0, zz]) + (c1[1, zz] + c1[2, zz])
        return 0
    lax.fori_loop(0, NZ, sum_c, 0)
    to_c2 = [net.copy(gc.at[y, x, z_of[d]], c2.at[d - 1], {Z: z_of[d]}) for d in range(1, NZ)]
    start_all(to_c2)

    wait_all(to_b1)
    def sum_b(zz, _):
        gb[y, x, zz] = (gb[y, x, zz] + b1[0, zz]) + (b1[1, zz] + b1[2, zz])
        return 0
    lax.fori_loop(0, NZ, sum_b, 0)
    to_b2 = [net.copy(gb.at[y, x, z_of[d]], b2.at[d - 1], {Z: z_of[d]}) for d in range(1, NZ)]
    start_all(to_b2)

    ring_a.finish()
    to_pa = [
        net.copy(ga.at[y_of[dy], x_of[dx], z], pa.at[i], {Y: y_of[dy], X: x_of[dx]})
        for i, (dy, dx) in enumerate(spots[1:])
    ]
    start_all(to_pa)

    mine = gath.at[x, z]

    def settle(own, arrived, low, width):
        total = own
        for d in range(arrived.shape[0]):
            total = total + arrived[d]
        mine[:, low : low + width] = total.astype(BF16)

    def block(at, low, high):
        return gath.at[at[0], at[1], :, low:high]

    def same(at, low, high, dev, source):
        held, coming = block(at, low, high), block(source, low, high)
        return net.copy(held, held, dev, coming)

    class Relay:
        def __init__(self, low, high):
            self.along_z = {d: same((x, z), low, high, {Z: z_of[d]}, (x, z_of[NZ - d])) for d in NEAR}
            self.along_x = [same((x, z), low, high, {X: x_of[e]}, (x_of[NX - e], z)) for e in (2, 1, 3)]
            self.on = {
                d: [
                    same((x, z_of[NZ - d]), low, high, {X: x_of[e]}, (x_of[NX - e], z_of[NZ - d]))
                    for e in (2, 1, 3)
                ]
                for d in NEAR
            }

        def start(self):
            start_all(self.along_z.values())
            start_all(self.along_x)

        def forward(self):
            for d in NEAR:
                self.along_z[d].wait()
                start_all(self.on[d])

        def finish(self):
            wait_all(self.along_x)
            for d in NEAR:
                wait_all(self.on[d])

    wait_all(to_c2)
    settle(gc[y, x, z], c2, WA + WB, WC)
    wait_all(to_b2)
    settle(gb[y, x, z], b2, WA, WB)
    relay_bc = Relay(WA, QN + KN)
    relay_bc.start()
    wait_all(to_pa)
    settle(ga[y, x, z], pa, 0, WA)
    p_x = [same((x, z), 0, WP, {X: x_of[d]}, (x_of[NX - d], z)) for d in (2, 1, 3)]
    start_all(p_x)
    relay_a = Relay(WP, WA)
    relay_a.start()
    every = slice(None)
    p_z = [same((every, z), 0, WP, {Z: z_of[d]}, (every, z_of[NZ - d])) for d in (4, 3, 5, 2, 6, 1, 7)]
    relay_bc.forward()
    wait_all(p_x)
    start_all(p_z)
    relay_a.forward()

    def tile(p):
        return gath[:, :, :, 128 * p : 128 * (p + 1)].reshape(NX * NZ * BLK, 128)

    def precondition(p):
        right = jnp.dot(tile(p), roots[p], preferred_element_type=F32).astype(BF16)
        left = ql_ref if p < QPAIRS else kl_ref
        part = jnp.dot(left[...], right, preferred_element_type=F32)
        pp[:, :, 128 * p : 128 * (p + 1)] = part.reshape(NY, BLK, 128)

    def to_owner(low, high):
        copies = [
            net.copy(pp.at[y_of[d], :, low:high], pr.at[d - 1, :, low:high], {Y: y_of[d]}) for d in (2, 1, 3)
        ]
        start_all(copies)
        return copies

    relay_bc.finish()
    for p in range(WA // 128, PAIRS):
        precondition(p)
    to_pr = to_owner(WA, QN + KN)
    relay_a.finish()
    wait_all(p_z)
    for p in range(WA // 128):
        precondition(p)
    to_pr += to_owner(0, WA)

    low_half = lax.broadcasted_iota(jnp.int32, (HEAD_DIM, 128), 1) < HEAD_DIM
    for p in range(PAIRS):
        both = lax.dot_general(tile(p), tile(p), (((0,), (0,)), ((), ())), preferred_element_type=F32)
        packed = jnp.where(low_half, both[0:HEAD_DIM], both[HEAD_DIM:])
        gp[:, p] = packed.reshape(NY, BLK, 128)

    rows = pl.ds(pl.multiple_of(y * BLK, BLK), BLK)
    wait_all(to_pr)
    pre = (pp[y] + pr[0]) + (pr[1] + pr[2])
    qm2 = MOMENT_DECAY * qm_ref[rows, :] + (1.0 - MOMENT_DECAY) * pre[:, :QN]
    km2 = MOMENT_DECAY * km_ref[rows, :] + (1.0 - MOMENT_DECAY) * pre[:, QN:]
    qw, kw = qw_ref[rows, :], kw_ref[rows, :]
    here = (y * NX + x) * NT + t
    plane[here] = jnp.concatenate(
        [lane_sums(v * v) for v in (qw, qm2, kw, km2)] + [jnp.zeros((4, 128), F32)], axis=0
    )
    mbuf[y, :, :QN] = qm2
    mbuf[y, :, QN:] = km2

    def slot_from(dy, dx, dt):
        return (y_of[(NY - dy) % NY] * NX + x_of[(NX - dx) % NX]) * NT + lax.rem(t + dt, NT)

    to_plane = [
        net.copy(
            plane.at[here], plane.at[here], {Y: y_of[dy], X: x_of[dx], T: lax.rem(t + dt, NT)},
            plane.at[slot_from(dy, dx, dt)],
        )
        for dy, dx, dt in others
    ]
    start_all(to_plane)
    to_m = [net.copy(mbuf.at[y], mbuf.at[y], {Y: y_of[d]}, mbuf.at[y_of[NY - d]]) for d in (1, 3, 2)]
    start_all(to_m)
    to_gr = [net.copy(gp.at[y_of[d]], gr.at[d - 1], {Y: y_of[d]}) for d in (1, 3, 2)]
    start_all(to_gr)
    wait_all(to_plane)
    total = plane[0]
    for i in range(1, NY * NX * NT):
        total = total + plane[i]
    zed[z] = total
    to_zed = [net.copy(zed.at[z], zed.at[z], {Z: z_of[d]}, zed.at[z_of[NZ - d]]) for d in (4, 3, 5, 2, 6, 1, 7)]
    start_all(to_zed)
    wait_all(to_zed)
    total = zed[0]
    for i in range(1, NZ):
        total = total + zed[i]
    total = jnp.sum(total, axis=1, keepdims=True)
    q_rate = LEARN_RATE * (jnp.sqrt(total[0:1]) / jnp.sqrt(total[1:2] + EPSILON))
    k_rate = LEARN_RATE * (jnp.sqrt(total[2:3]) / jnp.sqrt(total[3:4] + EPSILON))

    qcopy_ref[z, x, y] = (qw - q_rate * qm2).astype(BF16)
    kcopy_ref[z, x, y] = (kw - k_rate * km2).astype(BF16)

    def a_of(zi, xi, yi):
        return [qcopy_ref.at[zi, xi, yi, :, 0:WA]]

    def b_of(zi, xi, yi):
        return [qcopy_ref.at[zi, xi, yi, :, WA : WA + WB]]

    def c_of(zi, xi, yi):
        return [qcopy_ref.at[zi, xi, yi, :, WA + WB :], kcopy_ref.at[zi, xi, yi]]

    def spread(of, own, dev, source):
        return [net.copy(a, a, dev, b) for a, b in zip(of(*own), of(*source))]

    whole = slice(None)
    to_a, to_bz, to_cz, to_by, to_cx = [], [], [], [], []
    for dy, dx in spots[1:]:
        to_a += spread(a_of, (z, x, y), {Y: y_of[dy], X: x_of[dx]}, (z, x_of[(NX - dx) % NX], y_of[(NY - dy) % NY]))
    for d in (4, 3, 5, 2, 6, 1, 7):
        to_bz += spread(b_of, (z, x, y), {Z: z_of[d]}, (z_of[NZ - d], x, y))
        to_cz += spread(c_of, (z, x, y), {Z: z_of[d]}, (z_of[NZ - d], x, y))
    for d in (2, 1, 3):
        to_by += spread(b_of, (whole, x, y), {Y: y_of[d]}, (whole, x, y_of[NY - d]))
        to_cx += spread(c_of, (whole, x, y), {X: x_of[d]}, (whole, x_of[NX - d], y))
    ring_a = RingGather(net, Z, NZ, lambda c, h: a_of(c, pl.ds(2 * h, 2), whole))
    ring_b = RingGather(net, X, NX, lambda c, h: b_of(pl.ds(4 * h, 4), c, whole))
    ring_c = RingGather(net, Y, NY, lambda c, h: c_of(pl.ds(4 * h, 4), whole, c))

    start_all(to_a)
    start_all(to_bz)
    start_all(to_cz)
    wait_all(to_a)
    ring_a.send(0)
    ring_a.send(1)
    wait_all(to_bz)
    start_all(to_by)
    wait_all(to_cz)
    start_all(to_cx)

    wait_all(to_m)
    for yy in range(NY):
        at = slice(BLK * yy, BLK * (yy + 1))
        m = mbuf[yy, :, :QN]
        qm2_ref[at, :] = m
        qstep_ref[at, :] = q_rate * m
        qnext_ref[at, :] = qw_ref[at, :] - q_rate * m
        m = mbuf[yy, :, QN:]
        km2_ref[at, :] = m
        kstep_ref[at, :] = k_rate * m
        knext_ref[at, :] = kw_ref[at, :] - k_rate * m
    wait_all(to_gr)
    gfin[y] = (gp[y] + gr[0]) + (gr[1] + gr[2])
    to_gfin = [net.copy(gfin.at[y], gfin.at[y], {Y: y_of[d]}, gfin.at[y_of[NY - d]]) for d in (1, 3, 2)]

    ring_a.send(2)
    wait_all(to_by)
    ring_b.send(0)
    ring_b.send(1)
    ring_a.send(3)
    wait_all(to_cx)
    ring_c.send(0)
    ring_c.send(1)
    start_all(to_gfin)
    ring_a.send(4)
    ring_a.send(5)
    ring_b.send(2)
    ring_c.send(2)
    ring_a.send(6)

    wait_all(to_gfin)
    for p in range(PAIRS):
        source, target, h = (qs_ref, qs2_ref, 2 * p) if p < QPAIRS else (ks_ref, ks2_ref, 2 * (p - QPAIRS))
        gram = gfin[:, p].reshape(HEAD_DIM, 128) * ((1.0 - STAT_DECAY) / D)
        target[h] = STAT_DECAY * source[h] + gram[:, :HEAD_DIM]
        target[h + 1] = STAT_DECAY * source[h + 1] + gram[:, HEAD_DIM:]

    ring_b.finish()
    ring_c.finish()
    ring_a.finish()
    net.drain()


def write_kernel(*refs):
    n = len(refs) // 2
    sem = refs[-1]
    copies = [pltpu.make_async_copy(refs[i], refs[n + i], sem.at[i]) for i in range(n)]
    start_all(copies)
    wait_all(copies)


def shards(*args):
    hbm = pl.BlockSpec(memory_space=pltpu.HBM)
    space = pl.BlockSpec(memory_space=pltpu.VMEM)
    vm, dma = pltpu.VMEM, pltpu.SemaphoreType.DMA
    blocks = (NZ, NX, NY, BLK)
    outs = (
        ((64, QN), F32), ((64, KN), F32),
        ((64, QN), F32), ((64, KN), F32),
        ((*blocks, QN), BF16), ((*blocks, KN), BF16),
        ((64, QN), F32), ((64, KN), F32),
        ((16, 64, 64), F32), ((4, 64, 64), F32),
    )
    results = pl.pallas_call(
        step_kernel,
        out_shape=tuple(vm(*o) for o in outs),
        in_specs=[hbm] * 13,
        out_specs=[space] * 10,
        scratch_shapes=[
            vm((NY, NX, NZ, BLK, WA), F32),
            vm((NY, NX, NZ, BLK, WB), F32),
            vm((NY, NX, NZ, BLK, WC), F32),
            vm((2, 7, 2, NX, BLK, WA), F32),
            vm((2, 3, 2, NZ, BLK, WB), F32),
            vm((2, 3, 2, NZ, BLK, WC), F32),
            vm((15, BLK, WA), F32),
            vm((3, NZ, BLK, WB), F32),
            vm((3, NZ, BLK, WC), F32),
            vm((7, BLK, WB), F32),
            vm((7, BLK, WC), F32),
            vm((NX, NZ, BLK, QN + KN), BF16),
            vm((PAIRS, 128, 128), BF16),
            vm((NY, BLK, QN + KN), F32),
            vm((3, BLK, QN + KN), F32),
            vm((NY, BLK, QN + KN), F32),
            vm((NY, PAIRS, BLK, 128), F32),
            vm((3, PAIRS, BLK, 128), F32),
            vm((NY, PAIRS, BLK, 128), F32),
            vm((NY * NX * NT, 8, 128), F32),
            vm((NZ, 8, 128), F32),
            vm((NY, 1024, 512), BF16), vm((1024, QN), BF16), vm((1024, KN), BF16),
            vm((64, QN), F32), vm((64, KN), F32), vm((64, QN), F32), vm((64, KN), F32),
            vm((64, 512), BF16), vm((64, 512), BF16),
            vm((16, 64, 64), BF16), vm((4, 64, 64), BF16), vm((16, 64, 64), F32), vm((4, 64, 64), F32),
            dma((COPIES,)),
            dma((COPIES,)),
            dma((16,)),
        ],
        compiler_params=pltpu.CompilerParams(
            collective_id=0, has_side_effects=True, vmem_limit_bytes=46 * 2**20
        ),
        name="step",
    )(*(pltpu.with_memory_space_constraint(a, pltpu.HBM) for a in args))
    written = list(pl.pallas_call(
        write_kernel,
        out_shape=tuple(jax.ShapeDtypeStruct(*o) for o in outs),
        in_specs=[space] * 10,
        out_specs=[hbm] * 10,
        scratch_shapes=[dma((10,))],
        compiler_params=pltpu.CompilerParams(vmem_limit_bytes=2**20),
        name="write",
    )(*(pltpu.with_memory_space_constraint(r, pltpu.VMEM) for r in results)))
    written[4] = written[4].reshape(D, QN)
    written[5] = written[5].reshape(D, KN)
    return tuple(written)


def solution(mesh):
    split = Mesh(mesh.devices.reshape(NZ, NX, NY, NT), (Z, X, Y, T))
    row = P(FS, T)
    head = P(T, None, None)
    whole = P(None, T)
    tok = P(FS_REP, T)
    return jax.shard_map(
        shards, mesh=split,
        in_specs=(P(FS_REP, None), tok, tok, row, row, row, row, P(FS, None), P(FS, None), head, head, head, head),
        out_specs=(row, row, row, row, whole, whole, row, row, head, head),
        check_vma=False,
    )
```

```python
import jax
import jax.numpy as jnp
from jax import lax
from jax.experimental import pallas as pl
from jax.experimental.pallas import tpu as pltpu
from jax.sharding import Mesh
from jax.sharding import PartitionSpec as P

D = 2048
HEAD_DIM = 64
NZ, NX, NY, NT = 8, 4, 4, 2
Z, X, Y, T = "fs_0", "fs_1", "rep", "tp"
FS = (Z, X)
FS_REP = (Z, X, Y)
MOMENT_DECAY = 0.8
STAT_DECAY = 0.5
LEARN_RATE = 0.1
EPSILON = 1e-06
MESH = pl.DeviceIdType.MESH
QN, KN = 1024, 256
WA, WB, WC = 512, 384, 384
WP = 256
BLK = 16
PAIRS = 10
QPAIRS = 8
COPIES = 288
NEAR = (1, 7, 2, 6, 3, 5, 4)
F32, BF16 = jnp.float32, jnp.bfloat16


class Net:
    def __init__(self, send_sem, recv_sem):
        self.send_sem, self.recv_sem, self.used, self.sent = send_sem, recv_sem, 0, []

    def copy(self, src, dst, dev, landing=None):
        k = self.used
        self.used += 1
        copies = [
            pltpu.make_async_remote_copy(
                src_ref=a, dst_ref=b, send_sem=self.send_sem.at[k], recv_sem=self.recv_sem.at[k],
                device_id=dev, device_id_type=MESH,
            )
            for a, b in ((src, dst), (dst, dst) if landing is None else (landing, landing))
        ]
        return Copy(self, *copies)

    def drain(self):
        for copy in self.sent:
            copy.wait_send()


class Copy:
    def __init__(self, net, out, into):
        self.net, self.out, self.into = net, out, into

    def start(self):
        self.out.start()
        self.net.sent.append(self.out)

    def wait(self):
        self.into.wait_recv()


def start_all(copies):
    for copy in copies:
        copy.start()


def wait_all(copies):
    for copy in copies:
        copy.wait()


class Ring:
    def __init__(self, axis, n):
        self.n, self.me = n, lax.axis_index(axis)
        self.copies = {}
        self.device = [{axis: self.place(way, 1)} for way in range(2)]

    def place(self, way, dist):
        return lax.rem(self.me + (dist if way == 0 else self.n - dist), self.n)


class RingSum(Ring):
    def __init__(self, net, axis, n, region, recv, add):
        super().__init__(axis, n)
        self.recv, self.add = recv, add
        self.slots = [(n // 2, 0, None)]
        for k in range(1, n // 2):
            self.slots.append((n // 2 - k, 1, 2 * k - 3 if k >= 2 else None))
            self.slots.append((n // 2 - k, 0, 2 * k - 2))
        for way in range(2):
            for j, (dist, half, _) in enumerate(self.slots):
                self.copies[way, j] = net.copy(
                    region(self.place(way, dist), half ^ way), recv.at[way, j], self.device[way]
                )

    def send(self, j):
        for way in range(2):
            dist, half, source = self.slots[j]
            if source is not None:
                self.copies[way, source].wait()
                self.add(self.place(way, dist), half ^ way, self.recv.at[way, source])
            self.copies[way, j].start()

    def finish(self):
        for j in (self.n - 3, self.n - 2):
            for way in range(2):
                self.copies[way, j].wait()
                self.add(self.me, self.slots[j][1] ^ way, self.recv.at[way, j])


class RingGather(Ring):
    def __init__(self, net, axis, n, regions):
        super().__init__(axis, n)
        slots = [(j // 2, j % 2) for j in range(n - 1)]
        for way in range(2):
            for j, (k, half) in enumerate(slots):
                held = regions(self.place(1 - way, k), half ^ way)
                coming = regions(self.place(1 - way, k + 1), half ^ way)
                self.copies[way, j] = [
                    net.copy(a, a, self.device[way], b) for a, b in zip(held, coming)
                ]

    def send(self, j):
        for way in range(2):
            if j >= 2:
                wait_all(self.copies[way, j - 2])
            start_all(self.copies[way, j])

    def finish(self):
        for j in (self.n - 3, self.n - 2):
            for way in range(2):
                wait_all(self.copies[way, j])


def lane_sums(value):
    total = value[:, 0:128]
    for i in range(1, value.shape[1] // 128):
        total = total + value[:, 128 * i : 128 * (i + 1)]
    return jnp.sum(total, axis=0, keepdims=True)


def step_kernel(
    x_hbm, qc_hbm, kc_hbm, qw_hbm, kw_hbm, qm_hbm, km_hbm, ql_hbm, kl_hbm, qr_hbm, kr_hbm, qs_hbm, ks_hbm,
    qstep_ref, kstep_ref, qnext_ref, knext_ref, qcopy_ref, kcopy_ref, qm2_ref, km2_ref, qs2_ref, ks2_ref,
    ga, gb, gc, ra, rb, rc, pa, b1, c1, b2, c2,
    gath, roots, pp, pr, mbuf, gp, gr, gfin, plane, zed,
    x_ref, qc_ref, kc_ref, qw_ref, kw_ref, qm_ref, km_ref, ql_ref, kl_ref, qr_ref, kr_ref, qs_ref, ks_ref,
    send_sem, recv_sem, load_sem,
):
    z, x, y, t = (lax.axis_index(a) for a in (Z, X, Y, T))
    z_of = [lax.rem(z + d, NZ) for d in range(NZ)]
    x_of = [lax.rem(x + d, NX) for d in range(NX)]
    y_of = [lax.rem(y + d, NY) for d in range(NY)]
    spots = [(dy, dx) for dy in range(NY) for dx in range(NX)]
    spots.sort(key=lambda s: -min(s[0], NY - s[0]) - min(s[1], NX - s[1]))
    spots = [(0, 0)] + spots[:-1]
    others = [(dy, dx, dt) for dy, dx in spots for dt in range(NT) if dy or dx or dt]
    net = Net(send_sem, recv_sem)

    peers = [{Z: z_of[d]} for d in range(1, NZ)] + [
        {Y: y_of[dy], X: x_of[dx], T: lax.rem(t + dt, NT)} for dy, dx, dt in others
    ]
    barrier = pltpu.get_barrier_semaphore()
    for dev in peers:
        pl.semaphore_signal(barrier, inc=1, device_id=dev, device_id_type=MESH)

    l_at = pl.ds(pl.multiple_of(y * 512, 512), 512)
    loads = [(qc_hbm, qc_ref)]
    loads += [(x_hbm.at[:, 512 * i : 512 * (i + 1)], x_ref.at[i]) for i in range(NY)]
    loads += [(kc_hbm, kc_ref), (qr_hbm, qr_ref), (kr_hbm, kr_ref)]
    loads += [(ql_hbm.at[:, l_at], ql_ref), (kl_hbm.at[:, l_at], kl_ref)]
    loads += [(qw_hbm, qw_ref), (kw_hbm, kw_ref), (qm_hbm, qm_ref), (km_hbm, km_ref)]
    loads += [(qs_hbm, qs_ref), (ks_hbm, ks_ref)]
    loads = [pltpu.make_async_copy(a, b, load_sem.at[i]) for i, (a, b) in enumerate(loads)]
    start_all(loads)

    def product(rows, cot, low, width):
        return lax.dot_general(
            rows, cot[:, low : low + width], (((0,), (0,)), ((), ())), preferred_element_type=F32
        )

    def add_a(chunk, half, recv):
        for y2 in range(2):
            def body(x2, _):
                at = (2 * half + y2, x2, chunk)
                ga[at] = ga[at] + recv[y2, x2]
                return 0
            lax.fori_loop(0, NX, body, 0)

    def add_b(chunk, half, recv):
        for y2 in range(2):
            def body(z2, _):
                at = (2 * half + y2, chunk, z2)
                gb[at] = gb[at] + recv[y2, z2]
                return 0
            lax.fori_loop(0, NZ, body, 0)

    def add_c(chunk, half, recv):
        for x2 in range(2):
            def body(z2, _):
                at = (chunk, 2 * half + x2, z2)
                gc[at] = gc[at] + recv[x2, z2]
                return 0
            lax.fori_loop(0, NZ, body, 0)

    ring_a = RingSum(net, Z, NZ, lambda c, h: ga.at[pl.ds(2 * h, 2), :, c], ra, add_a)
    ring_b = RingSum(net, X, NX, lambda c, h: gb.at[pl.ds(2 * h, 2), c], rb, add_b)
    ring_c = RingSum(net, Y, NY, lambda c, h: gc.at[c, pl.ds(2 * h, 2)], rc, add_c)

    def make_b(chunk):
        at = pl.ds(pl.multiple_of(chunk * 128, 128), 128)
        rows = jnp.concatenate([x_ref[i, :, at] for i in range(NY)], axis=1)
        gb[:, chunk] = product(rows, qc_ref, WA, WB).reshape(NY, NZ, BLK, WB)

    def make_c(chunk):
        rows = x_ref[chunk]
        gc[chunk, :, :, :, 0:128] = product(rows, qc_ref, WA + WB, 128).reshape(NX, NZ, BLK, 128)
        gc[chunk, :, :, :, 128:WC] = product(rows, kc_ref, 0, KN).reshape(NX, NZ, BLK, KN)

    loads[0].wait()
    for i in range(NY):
        loads[1 + i].wait()
        ga[i] = product(x_ref[i], qc_ref, 0, WA).reshape(NX, NZ, BLK, WA)
    pl.semaphore_wait(barrier, len(peers))
    ring_a.send(0)
    ring_a.send(1)
    make_b(x_of[2])
    ring_b.send(0)
    for load in loads[1 + NY :]:
        load.wait()
    make_c(y_of[2])
    ring_c.send(0)
    make_b(x_of[1])
    make_b(x_of[3])
    ring_b.send(1)
    make_c(y_of[1])
    make_c(y_of[3])
    ring_c.send(1)
    ring_a.send(2)
    make_b(x_of[0])
    make_c(y_of[0])

    roots[...] = jnp.zeros_like(roots)
    for p in range(PAIRS):
        ref, h = (qr_ref, 2 * p) if p < QPAIRS else (kr_ref, 2 * (p - QPAIRS))
        roots[p, 0:HEAD_DIM, 0:HEAD_DIM] = ref[h]
        roots[p, HEAD_DIM : 2 * HEAD_DIM, HEAD_DIM : 2 * HEAD_DIM] = ref[h + 1]

    ring_a.send(3)
    ring_b.send(2)
    ring_c.send(2)
    ring_a.send(4)
    ring_a.send(5)
    ring_a.send(6)

    ring_c.finish()
    to_c1 = [net.copy(gc.at[y, x_of[d]], c1.at[d - 1], {X: x_of[d]}) for d in (1, 3, 2)]
    start_all(to_c1)
    ring_b.finish()
    to_b1 = [net.copy(gb.at[y_of[d], x], b1.at[d - 1], {Y: y_of[d]}) for d in (1, 3, 2)]
    start_all(to_b1)

    wait_all(to_c1)
    def sum_c(zz, _):
        gc[y, x, zz] = (gc[y, x, zz] + c1[0, zz]) + (c1[1, zz] + c1[2, zz])
        return 0
    lax.fori_loop(0, NZ, sum_c, 0)
    to_c2 = [net.copy(gc.at[y, x, z_of[d]], c2.at[d - 1], {Z: z_of[d]}) for d in range(1, NZ)]
    start_all(to_c2)

    ring_a.finish()
    to_pa = [
        net.copy(ga.at[y_of[dy], x_of[dx], z], pa.at[i], {Y: y_of[dy], X: x_of[dx]})
        for i, (dy, dx) in enumerate(spots[1:])
    ]
    start_all(to_pa)

    wait_all(to_b1)
    def sum_b(zz, _):
        gb[y, x, zz] = (gb[y, x, zz] + b1[0, zz]) + (b1[1, zz] + b1[2, zz])
        return 0
    lax.fori_loop(0, NZ, sum_b, 0)
    to_b2 = [net.copy(gb.at[y, x, z_of[d]], b2.at[d - 1], {Z: z_of[d]}) for d in range(1, NZ)]
    start_all(to_b2)

    mine = gath.at[x, z]

    def settle(own, arrived, low, width):
        total = own
        for d in range(arrived.shape[0]):
            total = total + arrived[d]
        mine[:, low : low + width] = total.astype(BF16)

    def block(at, low, high):
        return gath.at[at[0], at[1], :, low:high]

    def same(at, low, high, dev, source):
        held, coming = block(at, low, high), block(source, low, high)
        return net.copy(held, held, dev, coming)

    class Relay:
        def __init__(self, low, high):
            self.along_z = {d: same((x, z), low, high, {Z: z_of[d]}, (x, z_of[NZ - d])) for d in NEAR}
            self.along_x = [same((x, z), low, high, {X: x_of[e]}, (x_of[NX - e], z)) for e in (2, 1, 3)]
            self.on = {
                d: [
                    same((x, z_of[NZ - d]), low, high, {X: x_of[e]}, (x_of[NX - e], z_of[NZ - d]))
                    for e in (2, 1, 3)
                ]
                for d in NEAR
            }

        def start(self):
            start_all(self.along_z.values())
            start_all(self.along_x)

        def forward(self):
            for d in NEAR:
                self.along_z[d].wait()
                start_all(self.on[d])

        def finish(self):
            wait_all(self.along_x)
            for d in NEAR:
                wait_all(self.on[d])

    wait_all(to_c2)
    settle(gc[y, x, z], c2, WA + WB, WC)
    wait_all(to_b2)
    settle(gb[y, x, z], b2, WA, WB)
    relay_bc = Relay(WA, QN + KN)
    relay_bc.start()
    wait_all(to_pa)
    settle(ga[y, x, z], pa, 0, WA)
    p_x = [same((x, z), 0, WP, {X: x_of[d]}, (x_of[NX - d], z)) for d in (2, 1, 3)]
    start_all(p_x)
    relay_a = Relay(WP, WA)
    relay_a.start()
    every = slice(None)
    p_z = [same((every, z), 0, WP, {Z: z_of[d]}, (every, z_of[NZ - d])) for d in (4, 3, 5, 2, 6, 1, 7)]
    relay_bc.forward()
    wait_all(p_x)
    start_all(p_z)
    relay_a.forward()

    def tile(p):
        return gath[:, :, :, 128 * p : 128 * (p + 1)].reshape(NX * NZ * BLK, 128)

    def precondition(p):
        right = jnp.dot(tile(p), roots[p], preferred_element_type=F32).astype(BF16)
        left = ql_ref if p < QPAIRS else kl_ref
        part = jnp.dot(left[...], right, preferred_element_type=F32)
        pp[:, :, 128 * p : 128 * (p + 1)] = part.reshape(NY, BLK, 128)

    def to_owner(low, high):
        copies = [
            net.copy(pp.at[y_of[d], :, low:high], pr.at[d - 1, :, low:high], {Y: y_of[d]}) for d in (2, 1, 3)
        ]
        start_all(copies)
        return copies

    relay_bc.finish()
    for p in range(WA // 128, PAIRS):
        precondition(p)
    to_pr = to_owner(WA, QN + KN)
    relay_a.finish()
    wait_all(p_z)
    for p in range(WA // 128):
        precondition(p)
    to_pr += to_owner(0, WA)

    low_half = lax.broadcasted_iota(jnp.int32, (HEAD_DIM, 128), 1) < HEAD_DIM
    for p in range(PAIRS):
        both = lax.dot_general(tile(p), tile(p), (((0,), (0,)), ((), ())), preferred_element_type=F32)
        packed = jnp.where(low_half, both[0:HEAD_DIM], both[HEAD_DIM:])
        gp[:, p] = packed.reshape(NY, BLK, 128)

    rows = pl.ds(pl.multiple_of(y * BLK, BLK), BLK)
    wait_all(to_pr)
    pre = (pp[y] + pr[0]) + (pr[1] + pr[2])
    qm2 = MOMENT_DECAY * qm_ref[rows, :] + (1.0 - MOMENT_DECAY) * pre[:, :QN]
    km2 = MOMENT_DECAY * km_ref[rows, :] + (1.0 - MOMENT_DECAY) * pre[:, QN:]
    qw, kw = qw_ref[rows, :], kw_ref[rows, :]
    here = (y * NX + x) * NT + t
    plane[here] = jnp.concatenate(
        [lane_sums(v * v) for v in (qw, qm2, kw, km2)] + [jnp.zeros((4, 128), F32)], axis=0
    )
    mbuf[y, :, :QN] = qm2
    mbuf[y, :, QN:] = km2

    def slot_from(dy, dx, dt):
        return (y_of[(NY - dy) % NY] * NX + x_of[(NX - dx) % NX]) * NT + lax.rem(t + dt, NT)

    to_plane = [
        net.copy(
            plane.at[here], plane.at[here], {Y: y_of[dy], X: x_of[dx], T: lax.rem(t + dt, NT)},
            plane.at[slot_from(dy, dx, dt)],
        )
        for dy, dx, dt in others
    ]
    start_all(to_plane)
    to_m = [net.copy(mbuf.at[y], mbuf.at[y], {Y: y_of[d]}, mbuf.at[y_of[NY - d]]) for d in (1, 3, 2)]
    start_all(to_m)
    to_gr = [net.copy(gp.at[y_of[d]], gr.at[d - 1], {Y: y_of[d]}) for d in (1, 3, 2)]
    start_all(to_gr)
    wait_all(to_plane)
    total = plane[0]
    for i in range(1, NY * NX * NT):
        total = total + plane[i]
    zed[z] = total
    to_zed = [net.copy(zed.at[z], zed.at[z], {Z: z_of[d]}, zed.at[z_of[NZ - d]]) for d in (4, 3, 5, 2, 6, 1, 7)]
    start_all(to_zed)
    wait_all(to_zed)
    total = zed[0]
    for i in range(1, NZ):
        total = total + zed[i]
    total = jnp.sum(total, axis=1, keepdims=True)
    q_rate = LEARN_RATE * (jnp.sqrt(total[0:1]) / jnp.sqrt(total[1:2] + EPSILON))
    k_rate = LEARN_RATE * (jnp.sqrt(total[2:3]) / jnp.sqrt(total[3:4] + EPSILON))

    qcopy_ref[z, x, y] = (qw - q_rate * qm2).astype(BF16)
    kcopy_ref[z, x, y] = (kw - k_rate * km2).astype(BF16)

    def a_of(zi, xi, yi):
        return [qcopy_ref.at[zi, xi, yi, :, 0:WA]]

    def b_of(zi, xi, yi):
        return [qcopy_ref.at[zi, xi, yi, :, WA : WA + WB]]

    def c_of(zi, xi, yi):
        return [qcopy_ref.at[zi, xi, yi, :, WA + WB :], kcopy_ref.at[zi, xi, yi]]

    def spread(of, own, dev, source):
        return [net.copy(a, a, dev, b) for a, b in zip(of(*own), of(*source))]

    whole = slice(None)
    to_a, to_bz, to_cz, to_by, to_cx = [], [], [], [], []
    for dy, dx in spots[1:]:
        to_a += spread(a_of, (z, x, y), {Y: y_of[dy], X: x_of[dx]}, (z, x_of[(NX - dx) % NX], y_of[(NY - dy) % NY]))
    for d in (4, 3, 5, 2, 6, 1, 7):
        to_bz += spread(b_of, (z, x, y), {Z: z_of[d]}, (z_of[NZ - d], x, y))
        to_cz += spread(c_of, (z, x, y), {Z: z_of[d]}, (z_of[NZ - d], x, y))
    for d in (2, 1, 3):
        to_by += spread(b_of, (whole, x, y), {Y: y_of[d]}, (whole, x, y_of[NY - d]))
        to_cx += spread(c_of, (whole, x, y), {X: x_of[d]}, (whole, x_of[NX - d], y))
    ring_a = RingGather(net, Z, NZ, lambda c, h: a_of(c, pl.ds(2 * h, 2), whole))
    ring_b = RingGather(net, X, NX, lambda c, h: b_of(pl.ds(4 * h, 4), c, whole))
    ring_c = RingGather(net, Y, NY, lambda c, h: c_of(pl.ds(4 * h, 4), whole, c))

    start_all(to_a)
    start_all(to_bz)
    start_all(to_cz)
    wait_all(to_a)
    ring_a.send(0)
    ring_a.send(1)
    wait_all(to_bz)
    start_all(to_by)
    wait_all(to_cz)
    start_all(to_cx)

    wait_all(to_m)
    for yy in range(NY):
        at = slice(BLK * yy, BLK * (yy + 1))
        m = mbuf[yy, :, :QN]
        qm2_ref[at, :] = m
        qstep_ref[at, :] = q_rate * m
        qnext_ref[at, :] = qw_ref[at, :] - q_rate * m
        m = mbuf[yy, :, QN:]
        km2_ref[at, :] = m
        kstep_ref[at, :] = k_rate * m
        knext_ref[at, :] = kw_ref[at, :] - k_rate * m
    wait_all(to_gr)
    gfin[y] = (gp[y] + gr[0]) + (gr[1] + gr[2])
    to_gfin = [net.copy(gfin.at[y], gfin.at[y], {Y: y_of[d]}, gfin.at[y_of[NY - d]]) for d in (1, 3, 2)]

    ring_a.send(2)
    wait_all(to_by)
    ring_b.send(0)
    ring_b.send(1)
    ring_a.send(3)
    wait_all(to_cx)
    ring_c.send(0)
    ring_c.send(1)
    start_all(to_gfin)
    ring_a.send(4)
    ring_a.send(5)
    ring_b.send(2)
    ring_c.send(2)
    ring_a.send(6)

    wait_all(to_gfin)
    for p in range(PAIRS):
        source, target, h = (qs_ref, qs2_ref, 2 * p) if p < QPAIRS else (ks_ref, ks2_ref, 2 * (p - QPAIRS))
        gram = gfin[:, p].reshape(HEAD_DIM, 128) * ((1.0 - STAT_DECAY) / D)
        target[h] = STAT_DECAY * source[h] + gram[:, :HEAD_DIM]
        target[h + 1] = STAT_DECAY * source[h + 1] + gram[:, HEAD_DIM:]

    ring_b.finish()
    ring_c.finish()
    ring_a.finish()
    net.drain()


def write_kernel(*refs):
    n = len(refs) // 2
    sem = refs[-1]
    copies = [pltpu.make_async_copy(refs[i], refs[n + i], sem.at[i]) for i in range(n)]
    start_all(copies)
    wait_all(copies)


def shards(*args):
    hbm = pl.BlockSpec(memory_space=pltpu.HBM)
    space = pl.BlockSpec(memory_space=pltpu.VMEM)
    vm, dma = pltpu.VMEM, pltpu.SemaphoreType.DMA
    blocks = (NZ, NX, NY, BLK)
    outs = (
        ((64, QN), F32), ((64, KN), F32),
        ((64, QN), F32), ((64, KN), F32),
        ((*blocks, QN), BF16), ((*blocks, KN), BF16),
        ((64, QN), F32), ((64, KN), F32),
        ((16, 64, 64), F32), ((4, 64, 64), F32),
    )
    results = pl.pallas_call(
        step_kernel,
        out_shape=tuple(vm(*o) for o in outs),
        in_specs=[hbm] * 13,
        out_specs=[space] * 10,
        scratch_shapes=[
            vm((NY, NX, NZ, BLK, WA), F32),
            vm((NY, NX, NZ, BLK, WB), F32),
            vm((NY, NX, NZ, BLK, WC), F32),
            vm((2, 7, 2, NX, BLK, WA), F32),
            vm((2, 3, 2, NZ, BLK, WB), F32),
            vm((2, 3, 2, NZ, BLK, WC), F32),
            vm((15, BLK, WA), F32),
            vm((3, NZ, BLK, WB), F32),
            vm((3, NZ, BLK, WC), F32),
            vm((7, BLK, WB), F32),
            vm((7, BLK, WC), F32),
            vm((NX, NZ, BLK, QN + KN), BF16),
            vm((PAIRS, 128, 128), BF16),
            vm((NY, BLK, QN + KN), F32),
            vm((3, BLK, QN + KN), F32),
            vm((NY, BLK, QN + KN), F32),
            vm((NY, PAIRS, BLK, 128), F32),
            vm((3, PAIRS, BLK, 128), F32),
            vm((NY, PAIRS, BLK, 128), F32),
            vm((NY * NX * NT, 8, 128), F32),
            vm((NZ, 8, 128), F32),
            vm((NY, 1024, 512), BF16), vm((1024, QN), BF16), vm((1024, KN), BF16),
            vm((64, QN), F32), vm((64, KN), F32), vm((64, QN), F32), vm((64, KN), F32),
            vm((64, 512), BF16), vm((64, 512), BF16),
            vm((16, 64, 64), BF16), vm((4, 64, 64), BF16), vm((16, 64, 64), F32), vm((4, 64, 64), F32),
            dma((COPIES,)),
            dma((COPIES,)),
            dma((16,)),
        ],
        compiler_params=pltpu.CompilerParams(
            collective_id=0, has_side_effects=True, vmem_limit_bytes=46 * 2**20
        ),
        name="step",
    )(*(pltpu.with_memory_space_constraint(a, pltpu.HBM) for a in args))
    written = list(pl.pallas_call(
        write_kernel,
        out_shape=tuple(jax.ShapeDtypeStruct(*o) for o in outs),
        in_specs=[space] * 10,
        out_specs=[hbm] * 10,
        scratch_shapes=[dma((10,))],
        compiler_params=pltpu.CompilerParams(vmem_limit_bytes=2**20),
        name="write",
    )(*(pltpu.with_memory_space_constraint(r, pltpu.VMEM) for r in results)))
    written[4] = written[4].reshape(D, QN)
    written[5] = written[5].reshape(D, KN)
    return tuple(written)


def solution(mesh):
    split = Mesh(mesh.devices.reshape(NZ, NX, NY, NT), (Z, X, Y, T))
    row = P(FS, T)
    head = P(T, None, None)
    whole = P(None, T)
    tok = P(FS_REP, T)
    return jax.shard_map(
        shards, mesh=split,
        in_specs=(P(FS_REP, None), tok, tok, row, row, row, row, P(FS, None), P(FS, None), head, head, head, head),
        out_specs=(row, row, row, row, whole, whole, row, row, head, head),
        check_vma=False,
    )
```
